512 devices in a mesh: sp: 16 (over z), tp: 4 (over y), dp: 8 (over x, core).
Axes of the slice: x: 4, y: 4, z: 16, core: 2. Of those that a mesh axis runs over, the one named last changes fastest.
Arguments:
- latent: bfloat16 [8, 6144, 2048], P('dp', 'sp'), may hold values from -6 to 6
- conditioning: bfloat16 [8, 2048], P(None, 'sp'), may hold values from -6 to 6
- context_cond: bfloat16 [2048], P('sp'), may hold values from -6 to 6
- modulation: bfloat16 [3, 2048, 2048], P(None, 'sp', ('tp', 'dp')), may hold values from -4.2426407 to 4.2426407
- context: bfloat16 [8, 1024, 2048], P('dp', 'sp'), may hold values from -6 to 6
- query_weight: bfloat16 [2048, 1024], P(None, 'tp'), may hold values from -2.1213203 to 2.1213203
- key_projection: bfloat16 [2048, 256], P(None, 'tp'), may hold values from -0.13258252 to 0.13258252
- value_projection: bfloat16 [2048, 256], P(None, 'tp'), may hold values from -0.125 to 0.125
- out_weight: bfloat16 [1024, 2048], P(None, 'tp'), may hold values from -0.1875 to 0.1875
- sink_head_logit: float32 [16], P('tp'), may hold values from 5 to 7.5
- prefix_logit_bias: float32 [16], P('tp'), may hold values from -2.5 to -1
Outputs:
- updated: float32 [8, 6144, 2048], P('dp', 'sp', 'tp')
The draws below stay inside these ranges and needn't reach their ends.
All inputs are finite; a program needn't handle non-finite values.
Results may differ from the reference program's by a relative error of at most 0.0073.
Values may be sent and summed in bfloat16 or wider, within the bound.
A program may use at most 64 MiB of HBM per device.

```python
import jax
import jax.numpy as jnp
from jax import lax

MODEL_WIDTH = 2048
QUERY_HEADS = 16
KEY_VALUE_HEADS = 4
HEAD_SIZE = 64
GRID_W = 64
WINDOW_REACH = 128
SAMPLES = 8
LATENT_TOKENS = 6144
CONTEXT_TOKENS = 1024


def key_lookup_table(key):
    clip_bound = 6.0 * MODEL_WIDTH ** (-0.5)
    sampled_draws = jax.random.normal(jax.random.fold_in(key, 71), (MODEL_WIDTH, KEY_VALUE_HEADS * HEAD_SIZE), jnp.float32) * MODEL_WIDTH ** (-0.5)
    return jnp.clip(sampled_draws, -clip_bound, clip_bound)


def draw_key_projection(key, part):
    return key_lookup_table(key).astype(jnp.bfloat16)


def draw_query_weight(key, part):
    query_key = jax.random.fold_in(key, 72)
    clip_bound = 6.0 * MODEL_WIDTH ** (-0.5)
    sampled_draws = jax.random.normal(query_key, (MODEL_WIDTH, QUERY_HEADS * HEAD_SIZE), jnp.float32) * MODEL_WIDTH ** (-0.5)
    sampled_draws = jnp.clip(sampled_draws, -clip_bound, clip_bound)
    return sampled_draws.astype(jnp.bfloat16)


def draw_modulation(key, part):
    mod_key = jax.random.fold_in(key, 73)
    sampled_draws = jnp.clip(jax.random.normal(mod_key, (3, MODEL_WIDTH, MODEL_WIDTH), jnp.float32), -6.0, 6.0)
    boost = jnp.array([1.0, 1.0, 32.0], jnp.float32)[:, None, None]
    return (sampled_draws * boost * MODEL_WIDTH ** (-0.5)).astype(jnp.bfloat16)


def block_scale(rng, extent, cuts, low, largest):
    def one(position, shards_of):
        draws = jax.random.uniform(jax.random.fold_in(jax.random.fold_in(rng, 6), position), (shards_of,), jnp.float32, low / len(cuts), largest / len(cuts))
        return jnp.repeat(jnp.exp(draws), extent[position] // shards_of).reshape((-1,) + (1,) * (len(extent) - position - 1))

    factor_of = one(*cuts[0])
    for cut in cuts[1:]:
        factor_of = factor_of * one(*cut)
    return factor_of


def bell_draw(key, shape, deviation, limit, split=(), kind=jnp.bfloat16):
    drawn = jax.random.normal(key, shape, jnp.float32) * deviation
    if len(split) > 0:
        drawn = block_scale(key, shape, split, -0.22, 0.18) * drawn
    return jnp.clip(drawn, min=-limit, max=limit).astype(kind)


def setup_inputs(seed: int = 0) -> dict:
    key_list = jax.random.split(jax.random.key(seed), 12)
    latent = bell_draw(key_list[0], (SAMPLES, LATENT_TOKENS, MODEL_WIDTH), 1.0, 6.0, ((0, 8), (1, 16)))
    conditioning = bell_draw(key_list[1], (SAMPLES, MODEL_WIDTH), 1.0, 6.0, ((1, 16),))
    context_cond = bell_draw(key_list[2], (MODEL_WIDTH,), 1.0, 6.0, ((0, 16),))
    modulation = draw_modulation(jax.random.fold_in(key_list[11], 71), 0)
    context = bell_draw(key_list[4], (SAMPLES, CONTEXT_TOKENS, MODEL_WIDTH), 1.0, 6.0, ((0, 8), (1, 16)))
    query_weight = draw_query_weight(jax.random.fold_in(key_list[11], 71), 0)
    key_projection = draw_key_projection(jax.random.fold_in(key_list[11], 71), 0)
    value_projection = bell_draw(key_list[7], (MODEL_WIDTH, KEY_VALUE_HEADS * HEAD_SIZE), MODEL_WIDTH ** -0.5, 0.125, ((1, 4),))
    out_weight = bell_draw(key_list[8], (QUERY_HEADS * HEAD_SIZE, MODEL_WIDTH), (QUERY_HEADS * HEAD_SIZE) ** -0.5, 0.1875, ((1, 4),))
    sink_head_logit = jnp.clip(5.0 + 2.5 * jax.random.uniform(key_list[9], (QUERY_HEADS,), jnp.float32) ** block_scale(key_list[9], (QUERY_HEADS,), ((0, 4),), -0.2, 0.2), 5.0, 7.5)
    prefix_logit_bias = jnp.clip(-2.5 + 1.5 * jax.random.uniform(key_list[10], (QUERY_HEADS,), jnp.float32) ** block_scale(key_list[10], (QUERY_HEADS,), ((0, 4),), -0.2, 0.2), -2.5, -1.0)
    return {"latent": latent, "conditioning": conditioning, "context_cond": context_cond, "modulation": modulation, "context": context, "query_weight": query_weight, "key_projection": key_projection, "value_projection": value_projection, "out_weight": out_weight, "sink_head_logit": sink_head_logit, "prefix_logit_bias": prefix_logit_bias}


NORM_EPSILON = 1e-06
ROTARY_BASE = 10000.0
MASKED = -1e+30

def layer_norm(tok_rows):
    vectors = tok_rows.astype(jnp.float32)
    centre = lax.optimization_barrier(jnp.mean(vectors, axis=-1, keepdims=True))
    spread = lax.optimization_barrier(jnp.mean(jnp.square(vectors - centre), axis=-1, keepdims=True))
    return (vectors - centre) * lax.rsqrt(spread + NORM_EPSILON)

def turn_half(segment, token_positions):
    half_width = segment.shape[-1]
    quarter = half_width // 2
    frequency = ROTARY_BASE ** (-jnp.arange(0, half_width, 2, dtype=jnp.float32) / half_width)
    angles = token_positions.astype(jnp.float32)[:, None] * frequency[None, :]
    cosine = jnp.cos(angles)[:, None, :]
    sine_table = jnp.sin(angles)[:, None, :]
    leading = segment[..., :quarter]
    trailing = segment[..., quarter:]
    return jnp.concatenate([leading * cosine - trailing * sine_table, trailing * cosine + leading * sine_table], axis=-1)

def apply_rotary(head_rows, token_positions):
    half_width = head_rows.shape[-1] // 2
    return jnp.concatenate([turn_half(head_rows[..., :half_width], token_positions // GRID_W), turn_half(head_rows[..., half_width:], token_positions % GRID_W)], axis=-1)

def rounded_length(array):
    return lax.optimization_barrier(array.astype(jnp.bfloat16))

def reference(latent, conditioning, context_cond, modulation, context, query_weight, key_projection, value_projection, out_weight, sink_head_logit, prefix_logit_bias):
    cond_rows = jnp.concatenate([conditioning, context_cond[None, :]], axis=0)
    activated = jax.nn.silu(cond_rows.astype(jnp.float32)).astype(jnp.bfloat16)
    mod_all = jnp.stack([jnp.dot(activated, modulation[index], preferred_element_type=jnp.float32) for index in range(3)])
    ctx_shift = mod_all[0, -1]
    ctx_scale = mod_all[1, -1]
    heads_per_group = QUERY_HEADS // KEY_VALUE_HEADS
    block_list = LATENT_TOKENS // WINDOW_REACH
    factor = HEAD_SIZE ** (-0.5)
    token_positions = jnp.arange(LATENT_TOKENS, dtype=jnp.int32)
    block_start = jnp.arange(block_list, dtype=jnp.int32)[:, None] * WINDOW_REACH
    query_pos = block_start + jnp.arange(WINDOW_REACH, dtype=jnp.int32)[None, :]
    key_pos = block_start - WINDOW_REACH + jnp.arange(3 * WINDOW_REACH, dtype=jnp.int32)[None, :]
    inside = (key_pos >= 0) & (key_pos < LATENT_TOKENS)
    valid = (jnp.abs(query_pos[:, :, None] - key_pos[:, None, :]) <= WINDOW_REACH) & inside[:, None, :]
    head_bias_rows = prefix_logit_bias.astype(jnp.float32).reshape(KEY_VALUE_HEADS, heads_per_group)[:, :, None, None]
    sink_head_rows = sink_head_logit.astype(jnp.float32).reshape(KEY_VALUE_HEADS, heads_per_group)[:, :, None, None]

    def one_sample(operands):
        sample_rows, sample_ctx, mod_shift, mod_scale, mod_gate = operands
        normalized_input = (layer_norm(sample_rows) * (1.0 + mod_scale) + mod_shift).astype(jnp.bfloat16)
        ctx_normed = (layer_norm(sample_ctx) * (1.0 + ctx_scale) + ctx_shift).astype(jnp.bfloat16)
        query_rows = rounded_length(apply_rotary(jnp.dot(normalized_input, query_weight, preferred_element_type=jnp.float32).reshape(LATENT_TOKENS, QUERY_HEADS, HEAD_SIZE), token_positions))
        key_token_rows = rounded_length(apply_rotary(jnp.dot(normalized_input, key_projection, preferred_element_type=jnp.float32).reshape(LATENT_TOKENS, KEY_VALUE_HEADS, HEAD_SIZE), token_positions))
        value_token_rows = rounded_length(jnp.dot(normalized_input, value_projection, preferred_element_type=jnp.float32)).reshape(LATENT_TOKENS, KEY_VALUE_HEADS, HEAD_SIZE)
        prefix_keys = rounded_length(jnp.dot(ctx_normed, key_projection, preferred_element_type=jnp.float32))
        prefix_keys = prefix_keys.reshape(CONTEXT_TOKENS, KEY_VALUE_HEADS, HEAD_SIZE).astype(jnp.float32)
        prefix_values = rounded_length(jnp.dot(ctx_normed, value_projection, preferred_element_type=jnp.float32))
        prefix_values = prefix_values.reshape(CONTEXT_TOKENS, KEY_VALUE_HEADS, HEAD_SIZE).astype(jnp.float32)
        padding_amount = ((WINDOW_REACH, WINDOW_REACH), (0, 0), (0, 0))
        key_padded_rows = jnp.pad(key_token_rows, padding_amount).reshape(block_list + 2, WINDOW_REACH, KEY_VALUE_HEADS, HEAD_SIZE)
        value_padded_rows = jnp.pad(value_token_rows, padding_amount).reshape(block_list + 2, WINDOW_REACH, KEY_VALUE_HEADS, HEAD_SIZE)
        window_keys = jnp.concatenate([key_padded_rows[:-2], key_padded_rows[1:-1], key_padded_rows[2:]], axis=1).astype(jnp.float32)
        window_values = jnp.concatenate([value_padded_rows[:-2], value_padded_rows[1:-1], value_padded_rows[2:]], axis=1).astype(jnp.float32)
        query_block_list = query_rows.reshape(block_list, WINDOW_REACH, KEY_VALUE_HEADS, heads_per_group, HEAD_SIZE).astype(jnp.float32)

        def one_block(pieces):
            block_queries, block_keys, block_values, block_valid = pieces
            win_scores = jnp.einsum('qkgd,jkd->kgqj', block_queries, block_keys) * factor
            win_scores = jnp.where(block_valid[None, None], win_scores, MASKED)
            ctx_scores = jnp.einsum('qkgd,ckd->kgqc', block_queries, prefix_keys) * factor + head_bias_rows
            sink_scores = jnp.broadcast_to(sink_head_rows, win_scores.shape[:-1] + (1,))
            probs = jax.nn.softmax(jnp.concatenate([win_scores, ctx_scores, sink_scores], axis=-1), axis=-1)
            win_probs = rounded_length(probs[..., :3 * WINDOW_REACH]).astype(jnp.float32)
            ctx_probs = rounded_length(probs[..., 3 * WINDOW_REACH:3 * WINDOW_REACH + CONTEXT_TOKENS]).astype(jnp.float32)
            summed = jnp.einsum('kgqj,jkd->qkgd', win_probs, block_values) + jnp.einsum('kgqc,ckd->qkgd', ctx_probs, prefix_values)
            return summed.astype(jnp.bfloat16)
        attended = lax.map(one_block, (query_block_list, window_keys, window_values, valid))
        attended = attended.reshape(LATENT_TOKENS, QUERY_HEADS * HEAD_SIZE)
        mixed = jnp.dot(attended, out_weight, preferred_element_type=jnp.float32)
        return sample_rows.astype(jnp.float32) + mod_gate * mixed
    return lax.map(one_sample, (latent, context, mod_all[0, :-1], mod_all[1, :-1], mod_all[2, :-1]))
```

```python
import functools
import math

import jax
import jax.numpy as jnp
from jax import lax
from jax.experimental import pallas as pl
from jax.experimental.pallas import tpu as pltpu
from jax.sharding import PartitionSpec as P

HEAD = 64
GRID_W = 64
REACH = 128
EPS = 1e-06
BASE = 10000.0
MASKED = -1e30
LOG2E = math.log2(math.e)
F32 = jnp.float32
BF16 = jnp.bfloat16
LANES = 128
MESH = pl.DeviceIdType.MESH


def dot(a, b):
    return jnp.dot(a, b, preferred_element_type=F32)


def dot_t(a, b):
    return lax.dot_general(a, b, (((1,), (1,)), ((), ())), preferred_element_type=F32)


def lane_iota(shape):
    return lax.broadcasted_iota(jnp.int32, shape, len(shape) - 1)


def kernel(
    sizes,
    lat, cond, cctx, mod, ctx, qw, kw, vw, ow, sink, bias,
    out,
    xv, condv, cctxv, modv, cxv, qwv, kwv, vwv, owv, sinks, biass,
    zsend, zrecv, xysend, xyrecv, vecs,
    xn, cxn, xb, cxb, kvw, ct, st,
    kvc, kvx, qz, accw, mw, gath, outv,
    in_sems, out_sem,
    z_send, z_recv, xy_send, xy_recv, c_send, c_recv, h_send, h_recv, y_send, y_recv,
):
    SP, TP, DP = sizes
    T, D = xv.shape
    C = cxv.shape[0]
    samples = condv.shape[0]
    cols = owv.shape[1]
    width = qwv.shape[1]
    heads = width // HEAD
    blocks = T // REACH
    sp, tp, dp = lax.axis_index("sp"), lax.axis_index("tp"), lax.axis_index("dp")

    barrier = pltpu.get_barrier_semaphore()
    z_far = sorted(range(1, SP), key=lambda d: -min(d, SP - d))
    xy_off = [(t, d) for t in range(TP) for d in range(DP) if (t, d) != (0, 0)]
    for d in z_far:
        pl.semaphore_signal(barrier, inc=1, device_id={"sp": lax.rem(sp + d, SP)}, device_id_type=MESH)
    for t, d in xy_off:
        pl.semaphore_signal(
            barrier, inc=1, device_id={"tp": lax.rem(tp + t, TP), "dp": lax.rem(dp + d, DP)}, device_id_type=MESH
        )

    pairs = [(cond, condv), (cctx, cctxv), (mod, modv), (lat, xv), (ctx, cxv), (kw, kwv), (vw, vwv), (qw, qwv),
             (ow, owv), (sink, sinks), (bias, biass)]
    loads = []
    for i, (src, dst) in enumerate(pairs):
        copy = pltpu.make_async_copy(src, dst, in_sems.at[i])
        copy.start()
        loads.append(copy)

    loads[0].wait()
    loads[1].wait()
    loads[2].wait()
    act = jax.nn.silu(condv[...].astype(F32)).astype(BF16)
    act_c = jax.nn.silu(jnp.broadcast_to(cctxv[...].astype(F32), (8, cctxv.shape[1]))).astype(BF16)

    def packed(m):
        return dot(act, modv[m]), dot(act_c, modv[m])

    s0, c0 = packed(0)
    s1, c1 = packed(1)
    g2 = dot(act, modv[2])
    half = samples // 2
    main = jnp.concatenate([s0, s1], axis=1)
    side = jnp.concatenate([c0, c1], axis=1)
    gates = jnp.concatenate([g2[:half], g2[half:]], axis=1)
    zsend[0:samples, :] = main.astype(BF16)
    zsend[8:16, :] = jnp.concatenate([side[0:8 - half], gates], axis=0).astype(BF16)

    pl.semaphore_wait(barrier, len(z_far) + len(xy_off))

    sends = []
    for d in z_far:
        copy = pltpu.make_async_remote_copy(
            src_ref=zsend, dst_ref=zrecv.at[d - 1], send_sem=z_send, recv_sem=z_recv,
            device_id={"sp": lax.rem(sp + d, SP)}, device_id_type=MESH,
        )
        copy.start()

    loads[3].wait()

    def norm_rows(src, dst, rows):
        def step(i, _):
            r = pl.ds(pl.multiple_of(i * rows, rows), rows)
            v = src[r, :].astype(F32)
            v = v - jnp.mean(v, axis=-1, keepdims=True)
            dst[r, :] = v * lax.rsqrt(jnp.mean(v * v, axis=-1, keepdims=True) + EPS)
            return 0

        lax.fori_loop(0, src.shape[0] // rows, step, 0)

    norm_rows(xv, xn, 16)
    loads[4].wait()
    norm_rows(cxv, cxn, 16)
    loads[5].wait()
    loads[6].wait()
    kvw[...] = jnp.concatenate([kwv[...], vwv[...]], axis=1)
    kvc[:, LANES:] = jnp.ones((kvc.shape[0], LANES), BF16)
    kvx[:, LANES:] = jnp.ones((kvx.shape[0], LANES), BF16)

    lane = lane_iota((T, LANES))
    pos = lax.broadcasted_iota(jnp.int32, (T, LANES), 0) + sp * T
    inner = lane & 31
    freq = jnp.exp((inner & 15).astype(F32) * (-2.0 / 32.0 * math.log(BASE)))
    place = jnp.where((lane & 63) < 32, pos >> 6, pos & 63).astype(F32)
    angle = place * freq
    ct[...] = jnp.cos(angle)
    sine = jnp.sin(angle)
    st[...] = jnp.where(inner < 16, -sine, sine)

    pltpu.make_async_copy(zrecv, zrecv, z_recv).wait()
    total = zsend[...].astype(F32)
    for d in range(SP - 1):
        total = total + zrecv[d].astype(F32)
    odd = lax.rem(dp, 2)
    turned = pltpu.roll(total, 64, 1)
    here = jnp.where(odd == 0, total, turned)
    there = jnp.where(odd == 0, turned, total)
    keep = (lane_iota(total.shape) >> 6) == odd
    here = jnp.where(keep, here, 0.0)
    there = jnp.where(keep, there, 0.0)
    first_gate = 8 + 8 - half
    for s in range(samples):
        gate_rows = here if s < half else there
        row = first_gate + s % half
        xysend[s, 0:1, :] = here[s:s + 1]
        xysend[s, 1:2, :] = there[s:s + 1]
        xysend[s, 2:3, :] = here[8:9]
        xysend[s, 3:4, :] = there[8:9]
        xysend[s, 4:5, :] = gate_rows[row:row + 1]
    me = tp * DP + dp
    for t, d in xy_off:
        target = lax.rem(dp + d, DP)
        copy = pltpu.make_async_remote_copy(
            src_ref=xysend.at[target], dst_ref=xyrecv.at[me], send_sem=xy_send, recv_sem=xy_recv,
            device_id={"tp": lax.rem(tp + t, TP), "dp": target}, device_id_type=MESH,
        )
        copy.start()
    xyrecv[me] = xysend[dp]
    others = xyrecv.at[pl.ds(0, len(xy_off))]
    pltpu.make_async_copy(others, others, xy_recv).wait()
    chunks = vecs.shape[0]
    extra = jnp.where(lax.broadcasted_iota(jnp.int32, (8, LANES), 0) % 2 == 1, 1.0, 0.0)
    for k in range(chunks):
        vecs[k] = xyrecv[2 * k] + xyrecv[2 * k + 1] + extra

    def modulate(src, dst, shift_row):
        def step(k, _):
            c = pl.ds(pl.multiple_of(k * LANES, LANES), LANES)
            shift = vecs[k, shift_row:shift_row + 1, :]
            scale = vecs[k, shift_row + 1:shift_row + 2, :]
            dst[:, c] = (src[:, c] * scale + shift).astype(BF16)
            return 0

        lax.fori_loop(0, chunks, step, 0)

    modulate(cxn, cxb, 2)
    kvc[0:C, 0:LANES] = dot(cxb[...], kvw[...]).astype(BF16)
    for d in z_far:
        copy = pltpu.make_async_remote_copy(
            src_ref=kvc.at[pl.ds(0, C), pl.ds(0, LANES)], dst_ref=kvc.at[pl.ds(d * C, C), pl.ds(0, LANES)],
            send_sem=c_send, recv_sem=c_recv, device_id={"sp": lax.rem(sp + d, SP)}, device_id_type=MESH,
        )
        copy.start()

    modulate(xn, xb, 0)

    def partner(v):
        low = (lane_iota(v.shape) & 31) < 16
        return jnp.where(low, pltpu.roll(v, LANES - 16, 1), pltpu.roll(v, 16, 1))

    kv = dot(xb[...], kvw[...])
    is_key = lane_iota((T, LANES)) < 64
    kv = jnp.where(is_key, kv * ct[...] + partner(kv) * st[...], kv)
    kvx[REACH:REACH + T, 0:LANES] = kv.astype(BF16)
    before, after = lax.rem(sp + SP - 1, SP), lax.rem(sp + 1, SP)
    for side_index, (at, to, there_at) in enumerate(((T, after, 0), (REACH, before, REACH + T))):
        copy = pltpu.make_async_remote_copy(
            src_ref=kvx.at[pl.ds(at, REACH), pl.ds(0, LANES)], dst_ref=kvx.at[pl.ds(there_at, REACH), pl.ds(0, LANES)],
            send_sem=h_send.at[side_index], recv_sem=h_recv.at[side_index], device_id={"sp": to}, device_id_type=MESH,
        )
        copy.start()
        sends.append(copy)

    loads[7].wait()
    factor = LOG2E * HEAD ** (-0.5)
    low_lane = lane_iota((T, LANES)) < 64
    for j in range(width // LANES):
        q = dot(xb[...], qwv[:, j * LANES:(j + 1) * LANES])
        q = (q * ct[...] + partner(q) * st[...]) * factor
        qz[2 * j] = jnp.where(low_lane, q, 0.0).astype(BF16)
        qz[2 * j + 1] = jnp.where(low_lane, pltpu.roll(q, 64, 1), 0.0).astype(BF16)

    loads[9].wait()
    loads[10].wait()

    def per_head(ref):
        return jnp.concatenate([jnp.full((REACH, 1), ref[h] * LOG2E, F32) for h in range(heads)], axis=0)

    for copy in sends:
        copy.wait_recv()

    def window(b, _):
        r = pl.multiple_of(b * REACH, REACH)
        q = qz[:, pl.ds(r, REACH), :].reshape(heads * REACH, LANES)
        keys = kvx[pl.ds(r, 3 * REACH), :]
        s = dot_t(q, keys[:, 0:LANES])
        i = lax.broadcasted_iota(jnp.int32, (REACH, 3 * REACH), 0)
        j = lax.broadcasted_iota(jnp.int32, (REACH, 3 * REACH), 1)
        where = sp * T + r - REACH + j
        valid = (j >= i) & (j <= i + 2 * REACH) & (where >= 0) & (where < SP * T)
        s = jnp.where(valid[None], s.reshape(heads, REACH, 3 * REACH), MASKED).reshape(heads * REACH, 3 * REACH)
        m = jnp.max(s, axis=1, keepdims=True)
        accw[b] = dot(jnp.exp2(s - m).astype(BF16), keys)
        mw[b] = jnp.broadcast_to(m, (heads * REACH, LANES))
        return 0

    lax.fori_loop(0, blocks, window, 0)

    others = kvc.at[pl.ds(C, (SP - 1) * C), pl.ds(0, LANES)]
    pltpu.make_async_copy(others, others, c_recv).wait()

    def tp_copy(b, t, start):
        rows = pl.ds(b * REACH if isinstance(b, int) else pl.multiple_of(b * REACH, REACH), REACH)
        return pltpu.make_async_remote_copy(
            src_ref=gath.at[tp, rows], dst_ref=gath.at[tp, rows], send_sem=y_send.at[b, t - 1],
            recv_sem=y_recv.at[b, t - 1], device_id={"tp": lax.rem(tp + t, TP)}, device_id_type=MESH,
        )

    def context(b, _):
        r = pl.multiple_of(b * REACH, REACH)
        q = qz[:, pl.ds(r, REACH), :].reshape(heads * REACH, LANES)
        s = dot_t(q, kvc[:, 0:LANES])
        bias2 = per_head(biass)
        sink2 = per_head(sinks)
        m0 = mw[b][:, 0:1]
        m = jnp.maximum(jnp.maximum(m0, sink2), jnp.max(s, axis=1, keepdims=True) + bias2)
        acc = dot(jnp.exp2(s - (m - bias2)).astype(BF16), kvc[...])
        acc = acc + accw[b] * jnp.exp2(m0 - m)
        att = acc[:, 0:LANES] / (acc[:, LANES:] + jnp.exp2(sink2 - m))
        att = att.reshape(heads, REACH, LANES)
        low = lane_iota((REACH, LANES)) < 64
        for j in range(heads // 2):
            pair = jnp.where(low, pltpu.roll(att[2 * j], 64, 1), att[2 * j + 1])
            gath[tp, pl.ds(r, REACH), j * LANES:(j + 1) * LANES] = pair.astype(BF16)
        for t in range(1, TP):
            tp_copy(b, t, True).start()
        return 0

    lax.fori_loop(0, blocks, context, 0)

    loads[8].wait()
    gate = jnp.concatenate([vecs[tp * (cols // LANES) + j, 4:5, :] for j in range(cols // LANES)], axis=1)

    def project(b, _):
        r = pl.multiple_of(b * REACH, REACH)
        rows = pl.ds(r, REACH)
        for t in range(1, TP):
            tp_copy(b, t, False).wait_recv()
        mixed = dot(gath[0, rows, :], owv[0:width, :])
        for t in range(1, TP):
            mixed = mixed + dot(gath[t, rows, :], owv[t * width:(t + 1) * width, :])
        own = xv[rows, pl.ds(pl.multiple_of(tp * cols, LANES), cols)].astype(F32)
        outv[rows, :] = own + gate * mixed
        pltpu.make_async_copy(outv.at[rows], out.at[rows], out_sem.at[b]).start()
        return 0

    lax.fori_loop(0, blocks, project, 0)

    for b in range(blocks):
        pltpu.make_async_copy(outv.at[pl.ds(b * REACH, REACH)], out.at[pl.ds(b * REACH, REACH)], out_sem.at[b]).wait()
        for t in range(1, TP):
            tp_copy(b, t, False).wait_send()
    for copy in sends:
        copy.wait_send()
    pltpu.make_async_copy(zrecv, zrecv, z_send).wait()
    others = xyrecv.at[pl.ds(0, len(xy_off))]
    pltpu.make_async_copy(others, others, xy_send).wait()
    others = kvc.at[pl.ds(C, (SP - 1) * C), pl.ds(0, LANES)]
    pltpu.make_async_copy(others, others, c_send).wait()


def per_device(sizes, lat, cond, cctx, mod, ctx, qw, kw, vw, ow, sink, bias):
    SP, TP, DP = sizes
    T, D = lat.shape[1:]
    C = ctx.shape[1]
    width = qw.shape[1]
    heads = width // HEAD
    blocks = T // REACH
    cols = ow.shape[1]
    samples = cond.shape[0]
    any_space = pl.BlockSpec(memory_space=pl.ANY)
    vmem = pltpu.VMEM
    dma = pltpu.SemaphoreType.DMA
    scratch = [
        vmem((T, D), BF16), vmem(cond.shape, BF16), vmem((1, cctx.shape[0]), BF16), vmem(mod.shape, BF16),
        vmem((C, D), BF16), vmem(qw.shape, BF16), vmem(kw.shape, BF16), vmem(vw.shape, BF16), vmem(ow.shape, BF16),
        pltpu.SMEM(sink.shape, F32), pltpu.SMEM(bias.shape, F32),
        vmem((16, LANES), BF16), vmem((SP - 1, 16, LANES), BF16),
        vmem((samples, 8, LANES), F32), vmem((TP * DP, 8, LANES), F32), vmem((TP * DP // 2, 8, LANES), F32),
        vmem((T, D), F32), vmem((C, D), F32), vmem((T, D), BF16), vmem((C, D), BF16), vmem((D, LANES), BF16),
        vmem((T, LANES), F32), vmem((T, LANES), F32),
        vmem((SP * C, 2 * LANES), BF16), vmem((T + 2 * REACH, 2 * LANES), BF16), vmem((heads, T, LANES), BF16),
        vmem((blocks, heads * REACH, 2 * LANES), F32), vmem((blocks, heads * REACH, LANES), F32),
        vmem((TP, T, width), BF16), vmem((T, cols), F32),
        dma((11,)), dma((blocks,)),
        dma, dma, dma, dma, dma, dma, dma((2,)), dma((2,)), dma((blocks, TP - 1)), dma((blocks, TP - 1)),
    ]
    result = pl.pallas_call(
        functools.partial(kernel, sizes),
        out_shape=jax.ShapeDtypeStruct((T, cols), F32),
        in_specs=[any_space] * 11,
        out_specs=any_space,
        scratch_shapes=scratch,
        compiler_params=pltpu.CompilerParams(
            collective_id=0, has_side_effects=True, vmem_limit_bytes=60 * 1024 * 1024
        ),
        name="step",
    )(lat[0], cond, cctx[None, :], mod, ctx[0], qw, kw, vw, ow, sink, bias)
    return result[None]


def solution(mesh):
    placed = (
        P("dp", "sp", None),
        P(None, "sp"),
        P("sp"),
        P(None, "sp", ("tp", "dp")),
        P("dp", "sp", None),
        P(None, "tp"),
        P(None, "tp"),
        P(None, "tp"),
        P(None, "tp"),
        P("tp"),
        P("tp"),
    )
    sizes = (mesh.shape["sp"], mesh.shape["tp"], mesh.shape["dp"])
    return jax.shard_map(
        functools.partial(per_device, sizes),
        mesh=mesh, in_specs=placed, out_specs=P("dp", "sp", "tp"), check_vma=False,
    )
```

```python
import functools
import math

import jax
import jax.numpy as jnp
from jax import lax
from jax.experimental import pallas as pl
from jax.experimental.pallas import tpu as pltpu
from jax.sharding import PartitionSpec as P

HEAD = 64
GRID_W = 64
REACH = 128
EPS = 1e-06
BASE = 10000.0
MASKED = -1e30
LOG2E = math.log2(math.e)
F32 = jnp.float32
BF16 = jnp.bfloat16
LANES = 128
MESH = pl.DeviceIdType.MESH


def dot(a, b):
    return jnp.dot(a, b, preferred_element_type=F32)


def dot_t(a, b):
    return lax.dot_general(a, b, (((1,), (1,)), ((), ())), preferred_element_type=F32)


def full(v):
    return jnp.broadcast_to(v, (v.shape[0], LANES))


def wide(v, width):
    return jnp.concatenate([v] * (width // LANES), axis=1)


def lane_iota(shape):
    return lax.broadcasted_iota(jnp.int32, shape, len(shape) - 1)


DIRECT = (5, -5, 1, -1, 2, -2, -3)
RELAYED = (3, 4, 6, 7, 8, -4, -6, -7)
SLOT = {0: 0, **{d: i + 1 for i, d in enumerate((1, -1, 2, -2, -3, 5, -5) + RELAYED)}}
NEAR = 5


def kernel(
    sizes,
    lat, cond, cctx, mod, ctx, qw, kw, vw, ow, sink, bias,
    out,
    xv, condv, cctxv, modv, cxv, qwv, owv, sinks, biass,
    zsend, zrecv, xysend, xyrecv, vecs,
    xn, cxn, xb, cxb, kvw, ct, st,
    kvc, kvx, qz, accw, mw, gath, outv,
    in_sems, out_sem,
    z_send, z_recv, xy_send, xy_recv, c_send, c_recv, h_send, h_recv, y_send, y_recv,
):
    SP, TP, DP = sizes
    T, D = xv.shape
    C = cxv.shape[0]
    samples = condv.shape[0]
    cols = owv.shape[1]
    width = qwv.shape[1]
    heads = width // HEAD
    blocks = T // REACH
    sp, tp, dp = lax.axis_index("sp"), lax.axis_index("tp"), lax.axis_index("dp")

    def z_at(d):
        return {"sp": lax.rem(sp + d + SP, SP)}

    barrier = pltpu.get_barrier_semaphore()
    z_far = sorted(range(1, SP), key=lambda d: -min(d, SP - d))
    xy_off = [(t, d) for t in range(TP) for d in range(DP) if (t, d) != (0, 0)]
    for d in z_far:
        pl.semaphore_signal(barrier, inc=1, device_id=z_at(d), device_id_type=MESH)
    for t, d in xy_off:
        pl.semaphore_signal(
            barrier, inc=1, device_id={"tp": lax.rem(tp + t, TP), "dp": lax.rem(dp + d, DP)}, device_id_type=MESH
        )

    pairs = [(cond, condv), (cctx, cctxv), (mod, modv), (lat, xv), (ctx, cxv), (kw, kvw.at[0:HEAD]),
             (vw, kvw.at[HEAD:LANES]), (qw, qwv), (ow, owv), (sink, sinks), (bias, biass)]
    loads = []
    for i, (src, dst) in enumerate(pairs):
        copy = pltpu.make_async_copy(src, dst, in_sems.at[i])
        copy.start()
        loads.append(copy)

    loads[0].wait()
    loads[1].wait()
    loads[2].wait()
    act = jax.nn.silu(condv[...].astype(F32)).astype(BF16)
    act_c = jax.nn.silu(jnp.broadcast_to(cctxv[...].astype(F32), (8, cctxv.shape[1]))).astype(BF16)
    half = samples // 2
    weights = modv[...].reshape(-1, modv.shape[2])
    rows = dot_t(act, weights)
    side = dot_t(act_c, weights[0:LANES])
    gates = jnp.concatenate([rows[:half, LANES:], rows[half:, LANES:]], axis=1)
    zsend[0:samples, :] = rows[:, 0:LANES].astype(BF16)
    zsend[8:16, :] = jnp.concatenate([side[0:8 - half], gates], axis=0).astype(BF16)

    def norm_rows(src, dst, rows):
        def step(i, _):
            r = pl.ds(pl.multiple_of(i * rows, rows), rows)
            v = src[r, :].astype(F32)
            v = v - jnp.mean(v, axis=-1, keepdims=True)
            dst[r, :] = v * lax.rsqrt(jnp.mean(v * v, axis=-1, keepdims=True) + EPS)
            return 0

        lax.fori_loop(0, src.shape[0] // rows, step, 0)

    loads[3].wait()
    norm_rows(xv, xn, REACH)

    pl.semaphore_wait(barrier, len(z_far) + len(xy_off))
    for d in z_far:
        pltpu.make_async_remote_copy(
            src_ref=zsend, dst_ref=zrecv.at[d - 1], send_sem=z_send, recv_sem=z_recv,
            device_id=z_at(d), device_id_type=MESH,
        ).start()

    loads[4].wait()
    norm_rows(cxv, cxn, C)
    kvc[:, LANES:] = jnp.ones((kvc.shape[0], LANES), BF16)
    kvx[:, LANES:] = jnp.ones((kvx.shape[0], LANES), BF16)

    lane = lane_iota((T, LANES))
    pos = lax.broadcasted_iota(jnp.int32, (T, LANES), 0) + sp * T
    inner = lane & 31
    freq = jnp.exp((inner & 15).astype(F32) * (-2.0 / 32.0 * math.log(BASE)))
    place = jnp.where((lane & 63) < 32, pos >> 6, pos & 63).astype(F32)
    angle = place * freq
    ct[...] = jnp.cos(angle)
    sine = jnp.sin(angle)
    st[...] = jnp.where(inner < 16, -sine, sine)
    loads[5].wait()
    loads[6].wait()

    pltpu.make_async_copy(zrecv, zrecv, z_recv).wait()
    total = zsend[...].astype(F32)
    for d in range(SP - 1):
        total = total + zrecv[d].astype(F32)
    first_gate = 8 + 8 - half
    for s in range(samples):
        row = first_gate + s % half
        xysend[s, 0:1, :] = total[s:s + 1]
        xysend[s, 1:2, :] = total[8:9]
        xysend[s, 2:3, :] = total[row:row + 1]
        xysend[s, 3:4, :] = total[row:row + 1]
    me = tp * DP + dp
    for t, d in sorted(xy_off, key=lambda o: -(min(o[0], TP - o[0]) + min(o[1], DP - o[1]) // 2)):
        target = lax.rem(dp + d, DP)
        pltpu.make_async_remote_copy(
            src_ref=xysend.at[target], dst_ref=xyrecv.at[me], send_sem=xy_send, recv_sem=xy_recv,
            device_id={"tp": lax.rem(tp + t, TP), "dp": target}, device_id_type=MESH,
        ).start()
    xyrecv[me] = xysend[dp]
    others = xyrecv.at[pl.ds(0, len(xy_off))]
    pltpu.make_async_copy(others, others, xy_recv).wait()
    chunks = vecs.shape[1]
    low4 = lane_iota((4, LANES)) < 64
    extra = jnp.where(lax.broadcasted_iota(jnp.int32, (4, LANES), 0) < 2, 1.0, 0.0)
    for k in range(chunks):
        left, right = xyrecv[2 * k], xyrecv[2 * k + 1]
        vecs[0, k] = jnp.where(low4, left, pltpu.roll(right, 64, 1))
        vecs[1, k] = jnp.where(low4, pltpu.roll(left, 64, 1), right) + extra

    def modulate(src, dst, row):
        def step(k, _):
            c = pl.ds(pl.multiple_of(k * LANES, LANES), LANES)
            shift = vecs[0, k, row:row + 1, :]
            scale = vecs[1, k, row:row + 1, :]
            dst[:, c] = (src[:, c] * scale + shift).astype(BF16)
            return 0

        lax.fori_loop(0, chunks, step, 0)

    def ctx_at(d, count=1):
        return kvc.at[pl.ds(SLOT[d] * C, count * C), pl.ds(0, LANES)]

    def ctx_copy(slot_from, slot_to, d, sem):
        return pltpu.make_async_remote_copy(
            src_ref=ctx_at(slot_from), dst_ref=ctx_at(slot_to), send_sem=c_send, recv_sem=c_recv.at[sem],
            device_id=z_at(d), device_id_type=MESH,
        )

    modulate(cxn, cxb, 1)
    kvc[0:C, 0:LANES] = dot_t(cxb[...], kvw[...]).astype(BF16)
    for d in DIRECT:
        ctx_copy(0, d, d, {5: 1, -5: 2}.get(d, 0)).start()

    modulate(xn, xb, 0)

    def partner(v):
        low = (lane_iota(v.shape) & 31) < 16
        return jnp.where(low, pltpu.roll(v, LANES - 16, 1), pltpu.roll(v, 16, 1))

    kv = dot_t(xb[...], kvw[...])
    is_key = lane_iota((T, LANES)) < 64
    kv = jnp.where(is_key, kv * ct[...] + partner(kv) * st[...], kv)
    kvx[REACH:REACH + T, 0:LANES] = kv.astype(BF16)
    sends = []
    for side_index, (at, to, there_at) in enumerate(((T, 1, 0), (REACH, -1, REACH + T))):
        copy = pltpu.make_async_remote_copy(
            src_ref=kvx.at[pl.ds(at, REACH), pl.ds(0, LANES)], dst_ref=kvx.at[pl.ds(there_at, REACH), pl.ds(0, LANES)],
            send_sem=h_send.at[side_index], recv_sem=h_recv.at[side_index], device_id=z_at(to), device_id_type=MESH,
        )
        copy.start()
        sends.append(copy)

    loads[7].wait()
    factor = LOG2E * HEAD ** (-0.5)
    low_lane = lane_iota((T, LANES)) < 64
    for j in range(width // LANES):
        q = dot(xb[...], qwv[:, j * LANES:(j + 1) * LANES])
        q = (q * ct[...] + partner(q) * st[...]) * factor
        qz[2 * j] = jnp.where(low_lane, q, 0.0).astype(BF16)
        qz[2 * j + 1] = jnp.where(low_lane, pltpu.roll(q, 64, 1), 0.0).astype(BF16)

    loads[9].wait()
    loads[10].wait()

    def per_head(ref):
        return jnp.concatenate([jnp.full((REACH, LANES), ref[h] * LOG2E, F32) for h in range(heads)], axis=0)

    def queries(b):
        return qz[:, b * REACH:(b + 1) * REACH, :].reshape(heads * REACH, LANES)

    def window(b):
        keys = kvx[b * REACH:(b + 3) * REACH, :]
        s = dot_t(queries(b), keys[:, 0:LANES])
        i = lax.broadcasted_iota(jnp.int32, (REACH, 3 * REACH), 0)
        j = lax.broadcasted_iota(jnp.int32, (REACH, 3 * REACH), 1)
        valid = (j >= i) & (j <= i + 2 * REACH)
        if b == 0:
            valid = valid & (sp * T - REACH + j >= 0)
        if b == blocks - 1:
            valid = valid & (sp * T + (b - 1) * REACH + j < SP * T)
        s = jnp.where(valid[None], s.reshape(heads, REACH, 3 * REACH), MASKED).reshape(heads * REACH, 3 * REACH)
        m = full(jnp.max(s, axis=1, keepdims=True))
        accw[b] = dot(jnp.exp2(s - wide(m, 3 * REACH)).astype(BF16), keys)
        mw[b] = m

    pltpu.make_async_copy(ctx_at(5), ctx_at(5), c_recv.at[1]).wait()
    for slot_to, d in ((8, 3), (7, 2), (6, 1), (3, -2), (4, -1)):
        ctx_copy(5, slot_to, d, 3).start()
    pltpu.make_async_copy(ctx_at(-5), ctx_at(-5), c_recv.at[2]).wait()
    for slot_to, d in ((-7, -2), (-6, -1), (-4, 1)):
        ctx_copy(-5, slot_to, d, 3).start()
    for copy in sends:
        copy.wait_recv()
    pltpu.make_async_copy(ctx_at(1, NEAR), ctx_at(1, NEAR), c_recv.at[0]).wait()

    first_keys = (1 + len(DIRECT)) * C

    def context(b, keys, others):
        s = dot_t(queries(b), keys[:, 0:LANES])
        bias2 = per_head(biass)
        m0 = mw[b]
        m = jnp.maximum(m0, full(jnp.max(s, axis=1, keepdims=True)) + bias2)
        if others is not None:
            m = jnp.maximum(m, others)
        p = jnp.exp2(s - wide(m - bias2, keys.shape[0])).astype(BF16)
        return m, dot(p, keys) + accw[b] * wide(jnp.exp2(m0 - m), 2 * LANES)

    for b in range(blocks):
        window(b)
    for b in range(blocks):
        m, acc = context(b, kvc[0:first_keys, :], None)
        accw[b] = acc
        mw[b] = m

    rest = ctx_at(RELAYED[0], len(RELAYED))
    pltpu.make_async_copy(rest, rest, c_recv.at[3]).wait()

    def tp_copy(b, way):
        up = way in (0, 2)
        owner = tp if way < 2 else lax.rem(tp + (TP - 1 if up else 1), TP)
        rows = pl.ds(b * REACH + (REACH // 2 if way == 3 else 0), REACH // 2 if way >= 2 else REACH)
        return pltpu.make_async_remote_copy(
            src_ref=gath.at[owner, rows], dst_ref=gath.at[owner, rows], send_sem=y_send.at[b, way],
            recv_sem=y_recv.at[b, way], device_id={"tp": lax.rem(tp + (1 if up else TP - 1), TP)}, device_id_type=MESH,
        )

    for b in range(blocks):
        sink2 = per_head(sinks)
        m, acc = context(b, kvc[first_keys:, :], sink2)
        att = acc[:, 0:LANES] / (acc[:, LANES:] + jnp.exp2(sink2 - m))
        att = att.reshape(heads, REACH, LANES)
        low = lane_iota((REACH, LANES)) < 64
        for j in range(heads // 2):
            pair = jnp.where(low, pltpu.roll(att[2 * j], 64, 1), att[2 * j + 1])
            gath[tp, b * REACH:(b + 1) * REACH, j * LANES:(j + 1) * LANES] = pair.astype(BF16)
        tp_copy(b, 0).start()
        tp_copy(b, 1).start()

    for b in range(blocks):
        for way in (0, 1):
            tp_copy(b, way).wait_recv()
            tp_copy(b, way + 2).start()

    loads[8].wait()
    gate_rows = [tp * (cols // LANES) + j for j in range(cols // LANES)]
    gate = jnp.concatenate(
        [jnp.where(dp < half, vecs[0, k, 2:3, :], vecs[1, k, 2:3, :]) for k in gate_rows], axis=1
    )

    for b in range(blocks):
        rows = pl.ds(b * REACH, REACH)
        tp_copy(b, 2).wait_recv()
        tp_copy(b, 3).wait_recv()
        mixed = dot(gath[0, rows, :], owv[0:width, :])
        for t in range(1, TP):
            mixed = mixed + dot(gath[t, rows, :], owv[t * width:(t + 1) * width, :])
        own = xv[rows, pl.ds(pl.multiple_of(tp * cols, LANES), cols)].astype(F32)
        outv[rows, :] = own + gate * mixed
        pltpu.make_async_copy(outv.at[rows], out.at[rows], out_sem.at[b]).start()

    for b in range(blocks):
        pltpu.make_async_copy(outv.at[pl.ds(b * REACH, REACH)], out.at[pl.ds(b * REACH, REACH)], out_sem.at[b]).wait()
        for way in range(4):
            tp_copy(b, way).wait_send()
    for copy in sends:
        copy.wait_send()
    pltpu.make_async_copy(zrecv, zrecv, z_send).wait()
    others = xyrecv.at[pl.ds(0, len(xy_off))]
    pltpu.make_async_copy(others, others, xy_send).wait()
    others = kvc.at[pl.ds(C, (SP - 1) * C), pl.ds(0, LANES)]
    pltpu.make_async_copy(others, others, c_send).wait()


def per_device(sizes, lat, cond, cctx, mod, ctx, qw, kw, vw, ow, sink, bias):
    SP, TP, DP = sizes
    T, D = lat.shape[1:]
    C = ctx.shape[1]
    width = qw.shape[1]
    heads = width // HEAD
    blocks = T // REACH
    cols = ow.shape[1]
    samples = cond.shape[0]
    any_space = pl.BlockSpec(memory_space=pl.ANY)
    vmem = pltpu.VMEM
    dma = pltpu.SemaphoreType.DMA
    scratch = [
        vmem((T, D), BF16), vmem(cond.shape, BF16), vmem((1, cctx.shape[0]), BF16), vmem((mod.shape[0], mod.shape[2], mod.shape[1]), BF16),
        vmem((C, D), BF16), vmem(qw.shape, BF16), vmem(ow.shape, BF16),
        pltpu.SMEM(sink.shape, F32), pltpu.SMEM(bias.shape, F32),
        vmem((16, LANES), BF16), vmem((SP - 1, 16, LANES), BF16),
        vmem((samples, 4, LANES), F32), vmem((TP * DP, 4, LANES), F32), vmem((2, TP * DP // 2, 4, LANES), F32),
        vmem((T, D), F32), vmem((C, D), F32), vmem((T, D), BF16), vmem((C, D), BF16), vmem((LANES, D), BF16),
        vmem((T, LANES), F32), vmem((T, LANES), F32),
        vmem((SP * C, 2 * LANES), BF16), vmem((T + 2 * REACH, 2 * LANES), BF16), vmem((heads, T, LANES), BF16),
        vmem((blocks, heads * REACH, 2 * LANES), F32), vmem((blocks, heads * REACH, LANES), F32),
        vmem((TP, T, width), BF16), vmem((T, cols), F32),
        dma((11,)), dma((blocks,)),
        dma, dma, dma, dma, dma, dma((4,)), dma((2,)), dma((2,)), dma((blocks, 4)), dma((blocks, 4)),
    ]
    result = pl.pallas_call(
        functools.partial(kernel, sizes),
        out_shape=jax.ShapeDtypeStruct((T, cols), F32),
        in_specs=[any_space] * 11,
        out_specs=any_space,
        scratch_shapes=scratch,
        compiler_params=pltpu.CompilerParams(
            collective_id=0, has_side_effects=True, vmem_limit_bytes=60 * 1024 * 1024
        ),
        name="step",
    )(lat[0], cond, cctx[None, :], mod.transpose(0, 2, 1), ctx[0], qw, kw.T, vw.T, ow, sink, bias)
    return result[None]


def solution(mesh):
    placed = (
        P("dp", "sp", None),
        P(None, "sp"),
        P("sp"),
        P(None, "sp", ("tp", "dp")),
        P("dp", "sp", None),
        P(None, "tp"),
        P(None, "tp"),
        P(None, "tp"),
        P(None, "tp"),
        P("tp"),
        P("tp"),
    )
    sizes = (mesh.shape["sp"], mesh.shape["tp"], mesh.shape["dp"])
    return jax.shard_map(
        functools.partial(per_device, sizes),
        mesh=mesh, in_specs=placed, out_specs=P("dp", "sp", "tp"), check_vma=False,
    )
```

```python
import functools
import math

import jax
import jax.numpy as jnp
from jax import lax
from jax.experimental import pallas as pl
from jax.experimental.pallas import tpu as pltpu
from jax.sharding import PartitionSpec as P

HEAD = 64
GRID_W = 64
REACH = 128
EPS = 1e-06
BASE = 10000.0
MASKED = -1e30
LOG2E = math.log2(math.e)
F32 = jnp.float32
BF16 = jnp.bfloat16
LANES = 128
MESH = pl.DeviceIdType.MESH


def dot(a, b):
    return jnp.dot(a, b, preferred_element_type=F32)


def dot_t(a, b):
    return lax.dot_general(a, b, (((1,), (1,)), ((), ())), preferred_element_type=F32)


def full(v):
    return jnp.broadcast_to(v, (v.shape[0], LANES))


def wide(v, width):
    return jnp.concatenate([v] * (width // LANES), axis=1)


def lane_iota(shape):
    return lax.broadcasted_iota(jnp.int32, shape, len(shape) - 1)


DIRECT = (5, -5, 1, -1, 2, -2, -3)
NEAR = (1, -1, 2, -2, -3)
SOON = (4, 6, -4, -6)
LATE = (3, 7, 8, -7)
SLOT = {d: i for i, d in enumerate((0, *NEAR, 5, -5, *SOON, *LATE))}
PIECE = 128


def kernel(
    sizes,
    lat, cond, cctx, mod, ctx, qw, kw, vw, ow, sink, bias,
    out,
    xv, condv, cctxv, modv, cxv, qwv, owv, sinks, biass,
    zsend, zrecv, xysend, xyrecv, vecs,
    xn, cxn, xb, cxb, kvw, ct, st,
    kvc, kvx, qz, accw, mw, gath,
    in_sems,
    z_send, z_recv, xy_send, xy_recv, c_send, c_recv, h_send, h_recv, y_send, y_recv,
):
    SP, TP, DP = sizes
    T, D = xv.shape
    C = cxv.shape[0]
    samples = condv.shape[0]
    cols = owv.shape[1]
    width = qwv.shape[1]
    heads = width // HEAD
    blocks = T // REACH
    sp, tp, dp = lax.axis_index("sp"), lax.axis_index("tp"), lax.axis_index("dp")

    def z_at(d):
        return {"sp": lax.rem(sp + d + SP, SP)}

    barrier = pltpu.get_barrier_semaphore()
    z_far = sorted(range(1, SP), key=lambda d: -min(d, SP - d))
    xy_off = [(t, d) for t in range(TP) for d in range(DP) if (t, d) != (0, 0)]
    for d in z_far:
        pl.semaphore_signal(barrier, inc=1, device_id=z_at(d), device_id_type=MESH)
    for t, d in xy_off:
        pl.semaphore_signal(
            barrier, inc=1, device_id={"tp": lax.rem(tp + t, TP), "dp": lax.rem(dp + d, DP)}, device_id_type=MESH
        )

    pairs = [(cond, condv), (cctx, cctxv), (mod, modv), (lat, xv), (ctx, cxv), (kw, kvw.at[0:HEAD]),
             (vw, kvw.at[HEAD:LANES]), (qw, qwv), (ow, owv), (sink, sinks), (bias, biass)]
    loads = []
    for i, (src, dst) in enumerate(pairs):
        copy = pltpu.make_async_copy(src, dst, in_sems.at[i])
        copy.start()
        loads.append(copy)

    loads[0].wait()
    loads[1].wait()
    loads[2].wait()
    act = jax.nn.silu(condv[...].astype(F32)).astype(BF16)
    act_c = jax.nn.silu(jnp.broadcast_to(cctxv[...].astype(F32), (8, cctxv.shape[1]))).astype(BF16)
    half = samples // 2
    weights = modv[...].reshape(-1, modv.shape[2])
    rows = dot_t(act, weights)
    side = dot_t(act_c, weights[0:LANES])
    gates = jnp.concatenate([rows[:half, LANES:], rows[half:, LANES:]], axis=1)
    zsend[0:samples, :] = rows[:, 0:LANES].astype(BF16)
    zsend[8:16, :] = jnp.concatenate([side[0:8 - half], gates], axis=0).astype(BF16)

    def norm_rows(src, dst, rows):
        def step(i, _):
            r = pl.ds(pl.multiple_of(i * rows, rows), rows)
            v = src[r, :].astype(F32)
            v = v - jnp.mean(v, axis=-1, keepdims=True)
            dst[r, :] = v * lax.rsqrt(jnp.mean(v * v, axis=-1, keepdims=True) + EPS)
            return 0

        lax.fori_loop(0, src.shape[0] // rows, step, 0)

    loads[3].wait()
    norm_rows(xv, xn, REACH)

    pl.semaphore_wait(barrier, len(z_far) + len(xy_off))
    for d in z_far:
        pltpu.make_async_remote_copy(
            src_ref=zsend, dst_ref=zrecv.at[d - 1], send_sem=z_send, recv_sem=z_recv,
            device_id=z_at(d), device_id_type=MESH,
        ).start()

    loads[4].wait()
    norm_rows(cxv, cxn, C)
    kvc[:, LANES:] = jnp.ones((kvc.shape[0], LANES), BF16)
    kvx[:, LANES:] = jnp.ones((kvx.shape[0], LANES), BF16)

    lane = lane_iota((T, LANES))
    pos = lax.broadcasted_iota(jnp.int32, (T, LANES), 0) + sp * T
    inner = lane & 31
    freq = jnp.exp((inner & 15).astype(F32) * (-2.0 / 32.0 * math.log(BASE)))
    place = jnp.where((lane & 63) < 32, pos >> 6, pos & 63).astype(F32)
    angle = place * freq
    ct[...] = jnp.cos(angle)
    sine = jnp.sin(angle)
    st[...] = jnp.where(inner < 16, -sine, sine)
    loads[5].wait()
    loads[6].wait()

    pltpu.make_async_copy(zrecv, zrecv, z_recv).wait()
    total = zsend[...].astype(F32)
    for d in range(SP - 1):
        total = total + zrecv[d].astype(F32)
    first_gate = 8 + 8 - half
    for s in range(samples):
        row = first_gate + s % half
        xysend[s, 0:1, :] = total[s:s + 1]
        xysend[s, 1:2, :] = total[8:9]
        xysend[s, 2:3, :] = total[row:row + 1]
        xysend[s, 3:4, :] = total[row:row + 1]
    me = tp * DP + dp
    for t, d in sorted(xy_off, key=lambda o: -(min(o[0], TP - o[0]) + min(o[1], DP - o[1]) // 2)):
        target = lax.rem(dp + d, DP)
        pltpu.make_async_remote_copy(
            src_ref=xysend.at[target], dst_ref=xyrecv.at[me], send_sem=xy_send, recv_sem=xy_recv,
            device_id={"tp": lax.rem(tp + t, TP), "dp": target}, device_id_type=MESH,
        ).start()
    xyrecv[me] = xysend[dp]
    others = xyrecv.at[pl.ds(0, len(xy_off))]
    pltpu.make_async_copy(others, others, xy_recv).wait()
    chunks = vecs.shape[1]
    low4 = lane_iota((4, LANES)) < 64
    extra = jnp.where(lax.broadcasted_iota(jnp.int32, (4, LANES), 0) < 2, 1.0, 0.0)
    for k in range(chunks):
        left, right = xyrecv[2 * k], xyrecv[2 * k + 1]
        vecs[0, k] = jnp.where(low4, left, pltpu.roll(right, 64, 1))
        vecs[1, k] = jnp.where(low4, pltpu.roll(left, 64, 1), right) + extra

    def ctx_at(d, count=1):
        return kvc.at[pl.ds(SLOT[d] * C, count * C), pl.ds(0, LANES)]

    def ctx_copy(slot_from, slot_to, d, sem):
        return pltpu.make_async_remote_copy(
            src_ref=ctx_at(slot_from), dst_ref=ctx_at(slot_to), send_sem=c_send, recv_sem=c_recv.at[sem],
            device_id=z_at(d), device_id_type=MESH,
        )

    for k in range(chunks):
        c = slice(k * LANES, (k + 1) * LANES)
        cxb[:, c] = (cxn[:, c] * vecs[1, k, 1:2, :] + vecs[0, k, 1:2, :]).astype(BF16)
    kvc[0:C, 0:LANES] = dot_t(cxb[...], kvw[...]).astype(BF16)
    for d in DIRECT:
        ctx_copy(0, d, d, {5: 1, -5: 2}.get(d, 0)).start()

    def modulate(k, _):
        c = pl.ds(pl.multiple_of(k * LANES, LANES), LANES)
        xb[:, c] = (xn[:, c] * vecs[1, k, 0:1, :] + vecs[0, k, 0:1, :]).astype(BF16)
        return 0

    lax.fori_loop(0, chunks, modulate, 0)

    def partner(v):
        low = (lane_iota(v.shape) & 31) < 16
        return jnp.where(low, pltpu.roll(v, LANES - 16, 1), pltpu.roll(v, 16, 1))

    kv = dot_t(xb[...], kvw[...])
    is_key = lane_iota((T, LANES)) < 64
    kv = jnp.where(is_key, kv * ct[...] + partner(kv) * st[...], kv)
    kvx[REACH:REACH + T, 0:LANES] = kv.astype(BF16)
    sends = []
    for side_index, (at, to, there_at) in enumerate(((T, 1, 0), (REACH, -1, REACH + T))):
        copy = pltpu.make_async_remote_copy(
            src_ref=kvx.at[pl.ds(at, REACH), pl.ds(0, LANES)], dst_ref=kvx.at[pl.ds(there_at, REACH), pl.ds(0, LANES)],
            send_sem=h_send.at[side_index], recv_sem=h_recv.at[side_index], device_id=z_at(to), device_id_type=MESH,
        )
        copy.start()
        sends.append(copy)

    loads[7].wait()
    factor = LOG2E * HEAD ** (-0.5)
    low_lane = lane_iota((T, LANES)) < 64
    for j in range(width // LANES):
        q = dot(xb[...], qwv[:, j * LANES:(j + 1) * LANES])
        q = (q * ct[...] + partner(q) * st[...]) * factor
        qz[2 * j] = jnp.where(low_lane, q, 0.0).astype(BF16)
        qz[2 * j + 1] = jnp.where(low_lane, pltpu.roll(q, 64, 1), 0.0).astype(BF16)

    loads[9].wait()
    loads[10].wait()

    def per_head(ref, count):
        return jnp.concatenate([jnp.full((count, LANES), ref[h] * LOG2E, F32) for h in range(heads)], axis=0)

    def of_rows(ref, start, count):
        return ref[:, start:start + count, :].reshape(heads * count, ref.shape[2])

    def keep_state(start, count, m, acc):
        mw[:, start:start + count, :] = m.reshape(heads, count, LANES)
        accw[:, start:start + count, :] = acc.reshape(heads, count, 2 * LANES)

    def window(b):
        keys = kvx[b * REACH:(b + 3) * REACH, :]
        s = dot_t(of_rows(qz, b * REACH, REACH), keys[:, 0:LANES])
        i = lax.broadcasted_iota(jnp.int32, (REACH, 3 * REACH), 0)
        j = lax.broadcasted_iota(jnp.int32, (REACH, 3 * REACH), 1)
        valid = (j >= i) & (j <= i + 2 * REACH)
        if b == 0:
            valid = valid & (sp * T - REACH + j >= 0)
        if b == blocks - 1:
            valid = valid & (sp * T + (b - 1) * REACH + j < SP * T)
        s = jnp.where(valid[None], s.reshape(heads, REACH, 3 * REACH), MASKED).reshape(heads * REACH, 3 * REACH)
        m = full(jnp.max(s, axis=1, keepdims=True))
        keep_state(b * REACH, REACH, m, dot(jnp.exp2(s - wide(m, 3 * REACH)).astype(BF16), keys))

    def arrived(d, count, sem):
        blocks_here = ctx_at(d, count)
        pltpu.make_async_copy(blocks_here, blocks_here, c_recv.at[sem]).wait()

    def context(start, count, keys, others):
        s = dot_t(of_rows(qz, start, count), keys[:, 0:LANES])
        bias2 = per_head(biass, count)
        m0 = of_rows(mw, start, count)
        m = jnp.maximum(m0, full(jnp.max(s, axis=1, keepdims=True)) + bias2)
        if others is not None:
            m = jnp.maximum(m, others)
        p = jnp.exp2(s - wide(m - bias2, keys.shape[0])).astype(BF16)
        return m, dot(p, keys) + of_rows(accw, start, count) * wide(jnp.exp2(m0 - m), 2 * LANES)

    soon, late = SLOT[SOON[0]] * C, SLOT[LATE[0]] * C

    for b in range(1, blocks - 1):
        window(b)
    arrived(5, 1, 1)
    for slot_to, d in ((8, 3), (7, 2), (3, -2), (6, 1), (4, -1)):
        ctx_copy(5, slot_to, d, 4 if slot_to in LATE else 3).start()
    arrived(-5, 1, 2)
    for slot_to, d in ((-7, -2), (-6, -1), (-4, 1)):
        ctx_copy(-5, slot_to, d, 4 if slot_to in LATE else 3).start()
    for copy in sends:
        copy.wait_recv()
    arrived(NEAR[0], len(NEAR), 0)
    for b in (0, blocks - 1):
        window(b)
    for b in range(blocks):
        keep_state(b * REACH, REACH, *context(b * REACH, REACH, kvc[0:soon, :], None))
    arrived(SOON[0], len(SOON), 3)
    for b in range(blocks):
        keep_state(b * REACH, REACH, *context(b * REACH, REACH, kvc[soon:late, :], None))
    arrived(LATE[0], len(LATE), 4)

    def tp_copy(i, way):
        up = way in (0, 2)
        owner = tp if way < 2 else lax.rem(tp + (TP - 1 if up else 1), TP)
        rows = pl.ds(i * PIECE + (PIECE // 2 if way == 3 else 0), PIECE // 2 if way >= 2 else PIECE)
        return pltpu.make_async_remote_copy(
            src_ref=gath.at[owner, rows], dst_ref=gath.at[owner, rows], send_sem=y_send.at[i, way],
            recv_sem=y_recv.at[i, way], device_id={"tp": lax.rem(tp + (1 if up else TP - 1), TP)}, device_id_type=MESH,
        )

    pieces = T // PIECE
    sink2 = per_head(sinks, PIECE)
    low = lane_iota((PIECE, LANES)) < 64
    for i in range(pieces):
        m, acc = context(i * PIECE, PIECE, kvc[late:, :], sink2)
        att = acc[:, 0:LANES] / (acc[:, LANES:] + jnp.exp2(sink2 - m))
        att = att.reshape(heads, PIECE, LANES)
        for j in range(heads // 2):
            pair = jnp.where(low, pltpu.roll(att[2 * j], 64, 1), att[2 * j + 1])
            gath[tp, i * PIECE:(i + 1) * PIECE, j * LANES:(j + 1) * LANES] = pair.astype(BF16)
        tp_copy(i, 0).start()
        tp_copy(i, 1).start()

    for i in range(pieces):
        for way in (0, 1):
            tp_copy(i, way).wait_recv()
            tp_copy(i, way + 2).start()

    loads[8].wait()
    gate_rows = [tp * (cols // LANES) + j for j in range(cols // LANES)]
    gate = jnp.concatenate(
        [jnp.where(dp < half, vecs[0, k, 2:3, :], vecs[1, k, 2:3, :]) for k in gate_rows], axis=1
    )

    for b in range(blocks):
        rows = pl.ds(b * REACH, REACH)
        for i in range(b * REACH // PIECE, (b + 1) * REACH // PIECE):
            tp_copy(i, 2).wait_recv()
            tp_copy(i, 3).wait_recv()
        mixed = dot(gath[0, rows, :], owv[0:width, :])
        for t in range(1, TP):
            mixed = mixed + dot(gath[t, rows, :], owv[t * width:(t + 1) * width, :])
        own = xv[rows, pl.ds(pl.multiple_of(tp * cols, LANES), cols)].astype(F32)
        out[rows, :] = own + gate * mixed

    for i in range(pieces):
        for way in range(4):
            tp_copy(i, way).wait_send()
    for copy in sends:
        copy.wait_send()
    pltpu.make_async_copy(zrecv, zrecv, z_send).wait()
    others = xyrecv.at[pl.ds(0, len(xy_off))]
    pltpu.make_async_copy(others, others, xy_send).wait()
    others = kvc.at[pl.ds(C, (SP - 1) * C), pl.ds(0, LANES)]
    pltpu.make_async_copy(others, others, c_send).wait()


def per_device(sizes, lat, cond, cctx, mod, ctx, qw, kw, vw, ow, sink, bias):
    SP, TP, DP = sizes
    T, D = lat.shape[1:]
    C = ctx.shape[1]
    width = qw.shape[1]
    heads = width // HEAD
    blocks = T // REACH
    cols = ow.shape[1]
    samples = cond.shape[0]
    any_space = pl.BlockSpec(memory_space=pl.ANY)
    vmem = pltpu.VMEM
    dma = pltpu.SemaphoreType.DMA
    scratch = [
        vmem((T, D), BF16), vmem(cond.shape, BF16), vmem((1, cctx.shape[0]), BF16), vmem((mod.shape[0], mod.shape[2], mod.shape[1]), BF16),
        vmem((C, D), BF16), vmem(qw.shape, BF16), vmem(ow.shape, BF16),
        pltpu.SMEM(sink.shape, F32), pltpu.SMEM(bias.shape, F32),
        vmem((16, LANES), BF16), vmem((SP - 1, 16, LANES), BF16),
        vmem((samples, 4, LANES), F32), vmem((TP * DP, 4, LANES), F32), vmem((2, TP * DP // 2, 4, LANES), F32),
        vmem((T, D), F32), vmem((C, D), F32), vmem((T, D), BF16), vmem((C, D), BF16), vmem((LANES, D), BF16),
        vmem((T, LANES), F32), vmem((T, LANES), F32),
        vmem((SP * C, 2 * LANES), BF16), vmem((T + 2 * REACH, 2 * LANES), BF16), vmem((heads, T, LANES), BF16),
        vmem((heads, T, 2 * LANES), F32), vmem((heads, T, LANES), F32),
        vmem((TP, T, width), BF16),
        dma((11,)),
        dma, dma, dma, dma, dma, dma((5,)), dma((2,)), dma((2,)), dma((T // PIECE, 4)), dma((T // PIECE, 4)),
    ]
    result = pl.pallas_call(
        functools.partial(kernel, sizes),
        out_shape=vmem((T, cols), F32),
        in_specs=[any_space] * 11,
        out_specs=pl.BlockSpec(memory_space=vmem),
        scratch_shapes=scratch,
        compiler_params=pltpu.CompilerParams(
            collective_id=0, has_side_effects=True, vmem_limit_bytes=48 * 1024 * 1024
        ),
        name="step",
    )(*(pltpu.with_memory_space_constraint(v, pltpu.HBM) for v in (
        lat[0], cond, cctx[None, :], mod.transpose(0, 2, 1), ctx[0], qw, kw.T, vw.T, ow, sink, bias
    )))
    return result[None]


def solution(mesh):
    placed = (
        P("dp", "sp", None),
        P(None, "sp"),
        P("sp"),
        P(None, "sp", ("tp", "dp")),
        P("dp", "sp", None),
        P(None, "tp"),
        P(None, "tp"),
        P(None, "tp"),
        P(None, "tp"),
        P("tp"),
        P("tp"),
    )
    sizes = (mesh.shape["sp"], mesh.shape["tp"], mesh.shape["dp"])
    return jax.shard_map(
        functools.partial(per_device, sizes),
        mesh=mesh, in_specs=placed, out_specs=P("dp", "sp", "tp"), check_vma=False,
    )
```

```python
import functools
import math

import jax
import jax.numpy as jnp
from jax import lax
from jax.experimental import pallas as pl
from jax.experimental.pallas import tpu as pltpu
from jax.sharding import PartitionSpec as P

HEAD = 64
GRID_W = 64
REACH = 128
EPS = 1e-06
BASE = 10000.0
MASKED = -1e30
LOG2E = math.log2(math.e)
F32 = jnp.float32
BF16 = jnp.bfloat16
LANES = 128
MESH = pl.DeviceIdType.MESH


def dot(a, b):
    return jnp.dot(a, b, preferred_element_type=F32)


def dot_t(a, b):
    return lax.dot_general(a, b, (((1,), (1,)), ((), ())), preferred_element_type=F32)


def full(v):
    return jnp.broadcast_to(v, (v.shape[0], LANES))


def wide(v, width):
    return jnp.concatenate([v] * (width // LANES), axis=1)


def lane_iota(shape):
    return lax.broadcasted_iota(jnp.int32, shape, len(shape) - 1)


DIRECT = (5, -5, 1, -1, 2, -2, -3)
NEAR = (1, -1, 2, -2, -3)
SOON = (4, 6, -4, -6)
LATE = (3, 7, 8, -7)
SLOT = {d: i for i, d in enumerate((0, *NEAR, 5, -5, *SOON, *LATE))}
PIECE = 64
Z_ROWS = 10


def kernel(
    sizes,
    lat, cond, cctx, mod, ctx, qw, kw, vw, ow, sink, bias,
    out,
    xv, condv, cctxv, modv, cxv, qwv, owv, sinks, biass,
    zsend, zrecv, gsend, grecv, gsum, ghave, xysend, xyrecv, vecs,
    xn, cxn, xb, cxb, kvw, ct, st,
    kvc, kvx, qz, accw, mw, gath, mixed,
    in_sems,
    z_send, z_recv, xy_send, xy_recv, c_send, c_recv, h_send, h_recv, y_send, y_recv, g_sems,
):
    SP, TP, DP = sizes
    T, D = xv.shape
    C = cxv.shape[0]
    samples = condv.shape[0]
    cols = owv.shape[1]
    width = qwv.shape[1]
    heads = width // HEAD
    blocks = T // REACH
    sp, tp, dp = lax.axis_index("sp"), lax.axis_index("tp"), lax.axis_index("dp")

    def z_at(d):
        return {"sp": lax.rem(sp + d + SP, SP)}

    barrier = pltpu.get_barrier_semaphore()
    z_far = sorted(range(1, SP), key=lambda d: -min(d, SP - d))
    xy_off = [(t, d) for t in range(TP) for d in range(DP) if (t, d) != (0, 0)]
    for d in z_far:
        pl.semaphore_signal(barrier, inc=1, device_id=z_at(d), device_id_type=MESH)
    for t, d in xy_off:
        pl.semaphore_signal(
            barrier, inc=1, device_id={"tp": lax.rem(tp + t, TP), "dp": lax.rem(dp + d, DP)}, device_id_type=MESH
        )

    pairs = [(cond, condv), (cctx, cctxv), (mod, modv), (lat, xv), (ctx, cxv), (kw, kvw.at[0:HEAD]),
             (vw, kvw.at[HEAD:LANES]), (qw, qwv), (ow, owv), (sink, sinks), (bias, biass)]
    loads = []
    for i, (src, dst) in enumerate(pairs):
        copy = pltpu.make_async_copy(src, dst, in_sems.at[i])
        copy.start()
        loads.append(copy)

    loads[0].wait()
    loads[1].wait()
    loads[2].wait()
    act = jax.nn.silu(condv[...].astype(F32)).astype(BF16)
    act_c = jax.nn.silu(jnp.broadcast_to(cctxv[...].astype(F32), (8, cctxv.shape[1]))).astype(BF16)
    half = samples // 2
    weights = modv[...].reshape(-1, modv.shape[2])
    rows = dot_t(act, weights)
    side = dot_t(act_c, weights[0:LANES])
    zsend[0:samples, :] = rows[:, 0:LANES].astype(BF16)
    zsend[samples:, :] = side[0:Z_ROWS - samples].astype(BF16)
    gsend[...] = jnp.concatenate([rows[:half, LANES:], rows[half:, LANES:]], axis=1)

    def norm_rows(src, dst, rows):
        def step(i, _):
            r = pl.ds(pl.multiple_of(i * rows, rows), rows)
            v = src[r, :].astype(F32)
            v = v - jnp.mean(v, axis=-1, keepdims=True)
            dst[r, :] = v * lax.rsqrt(jnp.mean(v * v, axis=-1, keepdims=True) + EPS)
            return 0

        lax.fori_loop(0, src.shape[0] // rows, step, 0)

    pl.semaphore_wait(barrier, len(z_far) + len(xy_off))
    for d in z_far:
        pltpu.make_async_remote_copy(
            src_ref=zsend, dst_ref=zrecv.at[d - 1], send_sem=z_send, recv_sem=z_recv,
            device_id=z_at(d), device_id_type=MESH,
        ).start()

    loads[3].wait()
    norm_rows(xv, xn, REACH)
    loads[4].wait()
    norm_rows(cxv, cxn, C)
    kvc[:, LANES:] = jnp.ones((kvc.shape[0], LANES), BF16)
    kvx[:, LANES:] = jnp.ones((kvx.shape[0], LANES), BF16)

    lane = lane_iota((T, LANES))
    pos = lax.broadcasted_iota(jnp.int32, (T, LANES), 0) + sp * T
    inner = lane & 31
    freq = jnp.exp((inner & 15).astype(F32) * (-2.0 / 32.0 * math.log(BASE)))
    place = jnp.where((lane & 63) < 32, pos >> 6, pos & 63).astype(F32)
    angle = place * freq
    ct[...] = jnp.cos(angle)
    sine = jnp.sin(angle)
    st[...] = jnp.where(inner < 16, -sine, sine)
    loads[5].wait()
    loads[6].wait()

    pltpu.make_async_copy(zrecv, zrecv, z_recv).wait()
    total = zsend[...].astype(F32)
    for d in range(SP - 1):
        total = total + zrecv[d].astype(F32)
    for s in range(samples):
        xysend[s, 0:1, :] = total[s:s + 1]
        xysend[s, 1:2, :] = total[samples:samples + 1]
    me = tp * DP + dp
    for t, d in sorted(xy_off, key=lambda o: -(min(o[0], TP - o[0]) + min(o[1], DP - o[1]) // 2)):
        target = lax.rem(dp + d, DP)
        pltpu.make_async_remote_copy(
            src_ref=xysend.at[target], dst_ref=xyrecv.at[me], send_sem=xy_send, recv_sem=xy_recv,
            device_id={"tp": lax.rem(tp + t, TP), "dp": target}, device_id_type=MESH,
        ).start()
    xyrecv[me] = xysend[dp]
    for d in z_far:
        pltpu.make_async_remote_copy(
            src_ref=gsend, dst_ref=grecv.at[d - 1], send_sem=g_sems.at[0], recv_sem=g_sems.at[1],
            device_id=z_at(d), device_id_type=MESH,
        ).start()
    others = xyrecv.at[pl.ds(0, len(xy_off))]
    pltpu.make_async_copy(others, others, xy_recv).wait()
    chunks = vecs.shape[1]
    low2 = lane_iota((2, LANES)) < 64
    for k in range(chunks):
        left, right = xyrecv[2 * k], xyrecv[2 * k + 1]
        vecs[0, k] = jnp.where(low2, left, pltpu.roll(right, 64, 1))
        vecs[1, k] = jnp.where(low2, pltpu.roll(left, 64, 1), right) + 1.0

    def ctx_at(d, count=1):
        return kvc.at[pl.ds(SLOT[d] * C, count * C), pl.ds(0, LANES)]

    def ctx_copy(slot_from, slot_to, d, sem):
        return pltpu.make_async_remote_copy(
            src_ref=ctx_at(slot_from), dst_ref=ctx_at(slot_to), send_sem=c_send, recv_sem=c_recv.at[sem],
            device_id=z_at(d), device_id_type=MESH,
        )

    for k in range(chunks):
        c = slice(k * LANES, (k + 1) * LANES)
        cxb[:, c] = (cxn[:, c] * vecs[1, k, 1:2, :] + vecs[0, k, 1:2, :]).astype(BF16)
    kvc[0:C, 0:LANES] = dot_t(cxb[...], kvw[...]).astype(BF16)
    for d in DIRECT:
        ctx_copy(0, d, d, {5: 1, -5: 2}.get(d, 0)).start()

    def modulate(k, _):
        c = pl.ds(pl.multiple_of(k * LANES, LANES), LANES)
        xb[:, c] = (xn[:, c] * vecs[1, k, 0:1, :] + vecs[0, k, 0:1, :]).astype(BF16)
        return 0

    lax.fori_loop(0, chunks, modulate, 0)

    def partner(v):
        low = (lane_iota(v.shape) & 31) < 16
        return jnp.where(low, pltpu.roll(v, LANES - 16, 1), pltpu.roll(v, 16, 1))

    kv = dot_t(xb[...], kvw[...])
    is_key = lane_iota((T, LANES)) < 64
    kv = jnp.where(is_key, kv * ct[...] + partner(kv) * st[...], kv)
    kvx[REACH:REACH + T, 0:LANES] = kv.astype(BF16)
    sends = []
    for side_index, (at, to, there_at) in enumerate(((T, 1, 0), (REACH, -1, REACH + T))):
        copy = pltpu.make_async_remote_copy(
            src_ref=kvx.at[pl.ds(at, REACH), pl.ds(0, LANES)], dst_ref=kvx.at[pl.ds(there_at, REACH), pl.ds(0, LANES)],
            send_sem=h_send, recv_sem=h_recv.at[side_index], device_id=z_at(to), device_id_type=MESH,
        )
        copy.start()
        sends.append(copy)

    loads[7].wait()
    factor = LOG2E * HEAD ** (-0.5)
    low_lane = lane_iota((T, LANES)) < 64
    for j in range(width // LANES):
        q = dot(xb[...], qwv[:, j * LANES:(j + 1) * LANES])
        q = (q * ct[...] + partner(q) * st[...]) * factor
        qz[2 * j] = jnp.where(low_lane, q, 0.0).astype(BF16)
        qz[2 * j + 1] = jnp.where(low_lane, pltpu.roll(q, 64, 1), 0.0).astype(BF16)

    loads[9].wait()
    loads[10].wait()

    def per_head(ref, count):
        return jnp.concatenate([jnp.full((count, LANES), ref[h] * LOG2E, F32) for h in range(heads)], axis=0)

    def of_rows(ref, start, count):
        return ref[:, start:start + count, :].reshape(heads * count, ref.shape[2])

    def keep_state(start, count, m, acc):
        mw[:, start:start + count, :] = m.reshape(heads, count, LANES)
        accw[:, start:start + count, :] = acc.reshape(heads, count, 2 * LANES)

    def window(b):
        keys = kvx[b * REACH:(b + 3) * REACH, :]
        s = dot_t(of_rows(qz, b * REACH, REACH), keys[:, 0:LANES])
        i = lax.broadcasted_iota(jnp.int32, (REACH, 3 * REACH), 0)
        j = lax.broadcasted_iota(jnp.int32, (REACH, 3 * REACH), 1)
        valid = (j >= i) & (j <= i + 2 * REACH)
        if b == 0:
            valid = valid & (sp * T - REACH + j >= 0)
        if b == blocks - 1:
            valid = valid & (sp * T + (b - 1) * REACH + j < SP * T)
        s = jnp.where(valid[None], s.reshape(heads, REACH, 3 * REACH), MASKED).reshape(heads * REACH, 3 * REACH)
        m = full(jnp.max(s, axis=1, keepdims=True))
        keep_state(b * REACH, REACH, m, dot(jnp.exp2(s - wide(m, 3 * REACH)).astype(BF16), keys))

    def arrived(d, count, sem):
        blocks_here = ctx_at(d, count)
        pltpu.make_async_copy(blocks_here, blocks_here, c_recv.at[sem]).wait()

    def context(start, count, keys, others):
        s = dot_t(of_rows(qz, start, count), keys[:, 0:LANES])
        bias2 = per_head(biass, count)
        m0 = of_rows(mw, start, count)
        m = jnp.maximum(m0, full(jnp.max(s, axis=1, keepdims=True)) + bias2)
        if others is not None:
            m = jnp.maximum(m, others)
        p = jnp.exp2(s - wide(m - bias2, keys.shape[0])).astype(BF16)
        return m, dot(p, keys) + of_rows(accw, start, count) * wide(jnp.exp2(m0 - m), 2 * LANES)

    soon, late = SLOT[SOON[0]] * C, SLOT[LATE[0]] * C

    pltpu.make_async_copy(grecv, grecv, g_sems.at[1]).wait()
    gates = gsend[...]
    for d in range(SP - 1):
        gates = gates + grecv[d]
    gsum[...] = gates
    ghave[dp] = gates
    for d in range(1, DP):
        pltpu.make_async_remote_copy(
            src_ref=gsum, dst_ref=ghave.at[dp], send_sem=g_sems.at[2], recv_sem=g_sems.at[3],
            device_id={"dp": lax.rem(dp + d, DP)}, device_id_type=MESH,
        ).start()
    for b in range(1, blocks - 1):
        window(b)
    arrived(5, 1, 1)
    for slot_to, d in ((8, 3), (7, 2), (3, -2), (6, 1), (4, -1)):
        ctx_copy(5, slot_to, d, 4 if slot_to in LATE else 3).start()
    arrived(-5, 1, 2)
    for slot_to, d in ((-7, -2), (-6, -1), (-4, 1)):
        ctx_copy(-5, slot_to, d, 4 if slot_to in LATE else 3).start()
    for copy in sends:
        copy.wait_recv()
    arrived(NEAR[0], len(NEAR), 0)
    for b in (0, blocks - 1):
        window(b)
    for b in range(blocks):
        keep_state(b * REACH, REACH, *context(b * REACH, REACH, kvc[0:soon, :], None))
    arrived(SOON[0], len(SOON), 3)
    for b in range(blocks):
        keep_state(b * REACH, REACH, *context(b * REACH, REACH, kvc[soon:late, :], None))
    arrived(LATE[0], len(LATE), 4)

    def tp_copy(i, way):
        up = way in (0, 2)
        owner = tp if way < 2 else lax.rem(tp + (TP - 1 if up else 1), TP)
        rows = pl.ds(i * PIECE + (PIECE // 2 if way == 3 else 0), PIECE // 2 if way >= 2 else PIECE)
        return pltpu.make_async_remote_copy(
            src_ref=gath.at[owner, rows], dst_ref=gath.at[owner, rows], send_sem=y_send,
            recv_sem=y_recv.at[i, way], device_id={"tp": lax.rem(tp + (1 if up else TP - 1), TP)}, device_id_type=MESH,
        )

    pieces = T // PIECE
    sink2 = per_head(sinks, REACH)
    low = lane_iota((REACH, LANES)) < 64
    for b in range(blocks):
        m, acc = context(b * REACH, REACH, kvc[late:, :], sink2)
        att = acc[:, 0:LANES] / (acc[:, LANES:] + jnp.exp2(sink2 - m))
        att = att.reshape(heads, REACH, LANES)
        for j in range(heads // 2):
            pair = jnp.where(low, pltpu.roll(att[2 * j], 64, 1), att[2 * j + 1])
            gath[tp, b * REACH:(b + 1) * REACH, j * LANES:(j + 1) * LANES] = pair.astype(BF16)
        for i in range(b * REACH // PIECE, (b + 1) * REACH // PIECE):
            tp_copy(i, 0).start()
            tp_copy(i, 1).start()

    loads[8].wait()

    def projected(owner, rows):
        return dot(gath[owner, rows, :], owv[pl.ds(pl.multiple_of(owner * width, width), width), :])

    above, below, opposite = (lax.rem(tp + t, TP) for t in (1, TP - 1, 2))
    mixed[...] = projected(tp, pl.ds(0, T))
    for b in range(blocks):
        for i in range(b * REACH // PIECE, (b + 1) * REACH // PIECE):
            for way in (0, 1):
                tp_copy(i, way).wait_recv()
                tp_copy(i, way + 2).start()
        rows = pl.ds(b * REACH, REACH)
        mixed[rows, :] = mixed[rows, :] + projected(above, rows) + projected(below, rows)

    others = ghave.at[pl.ds(0, DP - 1)]
    pltpu.make_async_copy(others, others, g_sems.at[3]).wait()
    low1 = lane_iota((1, LANES)) < 64
    gate_chunks = []
    for k in range(DP // 2):
        left, right = (ghave[2 * k + i, pl.ds(lax.rem(dp, half), 1), :] for i in range(2))
        gate_chunks.append(jnp.where(
            dp < half,
            jnp.where(low1, left, pltpu.roll(right, 64, 1)),
            jnp.where(low1, pltpu.roll(left, 64, 1), right),
        ))
    gate = jnp.concatenate(gate_chunks, axis=1)
    for b in range(blocks):
        rows = pl.ds(b * REACH, REACH)
        for i in range(b * REACH // PIECE, (b + 1) * REACH // PIECE):
            tp_copy(i, 2).wait_recv()
            tp_copy(i, 3).wait_recv()
        own = xv[rows, pl.ds(pl.multiple_of(tp * cols, LANES), cols)].astype(F32)
        out[rows, :] = own + gate * (mixed[rows, :] + projected(opposite, rows))

    others = gath.at[pl.ds(0, TP - 1)]
    pltpu.make_async_copy(others, others, y_send).wait()
    others = kvx.at[pl.ds(0, 2 * REACH), pl.ds(0, LANES)]
    pltpu.make_async_copy(others, others, h_send).wait()
    pltpu.make_async_copy(zrecv, zrecv, z_send).wait()
    pltpu.make_async_copy(grecv, grecv, g_sems.at[0]).wait()
    others = ghave.at[pl.ds(0, DP - 1)]
    pltpu.make_async_copy(others, others, g_sems.at[2]).wait()
    others = xyrecv.at[pl.ds(0, len(xy_off))]
    pltpu.make_async_copy(others, others, xy_send).wait()
    others = kvc.at[pl.ds(C, (SP - 1) * C), pl.ds(0, LANES)]
    pltpu.make_async_copy(others, others, c_send).wait()


def per_device(sizes, lat, cond, cctx, mod, ctx, qw, kw, vw, ow, sink, bias):
    SP, TP, DP = sizes
    T, D = lat.shape[1:]
    C = ctx.shape[1]
    width = qw.shape[1]
    heads = width // HEAD
    blocks = T // REACH
    cols = ow.shape[1]
    samples = cond.shape[0]
    any_space = pl.BlockSpec(memory_space=pl.ANY)
    vmem = pltpu.VMEM
    dma = pltpu.SemaphoreType.DMA
    scratch = [
        vmem((T, D), BF16), vmem(cond.shape, BF16), vmem((1, cctx.shape[0]), BF16), vmem((mod.shape[0], mod.shape[2], mod.shape[1]), BF16),
        vmem((C, D), BF16), vmem(qw.shape, BF16), vmem(ow.shape, BF16),
        pltpu.SMEM(sink.shape, F32), pltpu.SMEM(bias.shape, F32),
        vmem((Z_ROWS, LANES), BF16), vmem((SP - 1, Z_ROWS, LANES), BF16),
        vmem((samples // 2, LANES), F32), vmem((SP - 1, samples // 2, LANES), F32), vmem((samples // 2, LANES), F32),
        vmem((DP, samples // 2, LANES), F32),
        vmem((samples, 2, LANES), F32), vmem((TP * DP, 2, LANES), F32), vmem((2, TP * DP // 2, 2, LANES), F32),
        vmem((T, D), F32), vmem((C, D), F32), vmem((T, D), BF16), vmem((C, D), BF16), vmem((LANES, D), BF16),
        vmem((T, LANES), F32), vmem((T, LANES), F32),
        vmem((SP * C, 2 * LANES), BF16), vmem((T + 2 * REACH, 2 * LANES), BF16), vmem((heads, T, LANES), BF16),
        vmem((heads, T, 2 * LANES), F32), vmem((heads, T, LANES), F32),
        vmem((TP, T, width), BF16), vmem((T, cols), F32),
        dma((11,)),
        dma, dma, dma, dma, dma, dma((5,)), dma, dma((2,)), dma, dma((T // PIECE, 4)), dma((4,)),
    ]
    result = pl.pallas_call(
        functools.partial(kernel, sizes),
        out_shape=vmem((T, cols), F32),
        in_specs=[any_space] * 11,
        out_specs=pl.BlockSpec(memory_space=vmem),
        scratch_shapes=scratch,
        compiler_params=pltpu.CompilerParams(
            collective_id=0, has_side_effects=True, vmem_limit_bytes=48 * 1024 * 1024
        ),
        name="step",
    )(*(pltpu.with_memory_space_constraint(v, pltpu.HBM) for v in (
        lat[0], cond, cctx[None, :], mod.transpose(0, 2, 1), ctx[0], qw, kw.T, vw.T, ow, sink, bias
    )))
    return result[None]


def solution(mesh):
    placed = (
        P("dp", "sp", None),
        P(None, "sp"),
        P("sp"),
        P(None, "sp", ("tp", "dp")),
        P("dp", "sp", None),
        P(None, "tp"),
        P(None, "tp"),
        P(None, "tp"),
        P(None, "tp"),
        P("tp"),
        P("tp"),
    )
    sizes = (mesh.shape["sp"], mesh.shape["tp"], mesh.shape["dp"])
    return jax.shard_map(
        functools.partial(per_device, sizes),
        mesh=mesh, in_specs=placed, out_specs=P("dp", "sp", "tp"), check_vma=False,
    )
```

```python
import functools
import math

import jax
import jax.numpy as jnp
from jax import lax
from jax.experimental import pallas as pl
from jax.experimental.pallas import tpu as pltpu
from jax.sharding import PartitionSpec as P

HEAD = 64
GRID_W = 64
REACH = 128
EPS = 1e-06
BASE = 10000.0
MASKED = -1e30
LOG2E = math.log2(math.e)
F32 = jnp.float32
BF16 = jnp.bfloat16
LANES = 128
MESH = pl.DeviceIdType.MESH


def dot(a, b):
    return jnp.dot(a, b, preferred_element_type=F32)


def dot_t(a, b):
    return lax.dot_general(a, b, (((1,), (1,)), ((), ())), preferred_element_type=F32)


def full(v):
    return jnp.broadcast_to(v, (v.shape[0], LANES))


def wide(v, width):
    return jnp.concatenate([v] * (width // LANES), axis=1)


def lane_iota(shape):
    return lax.broadcasted_iota(jnp.int32, shape, len(shape) - 1)


DIRECT = (5, -5, 1, -1, 2, -2, -3)
NEAR = (1, -1, 2, -2, -3)
SOON = (4, 6, -4, -6)
LATE = (3, 7, 8, -7)
SLOT = {d: i for i, d in enumerate((0, *NEAR, 5, -5, *SOON, *LATE))}
PIECE = 64


def kernel(
    sizes,
    lat, cond, cctx, mod, ctx, qw, kw, vw, ow, sink, bias,
    out,
    xv, condv, cctxv, modv, cxv, qwv, owv, sinks, biass,
    zsend, zcsend, zrecv, zcrecv, gsend, grecv, gsum, ghave, xysend, xyrecv, vecs,
    xn, cxn, xb, cxb, kvw, ct, st,
    kvc, kvx, qz, accw, mw, gath, mixed,
    in_sems,
    z_send, z_recv, xy_send, xy_recv, c_send, c_recv, h_send, h_recv, y_send, y_recv, g_sems,
):
    SP, TP, DP = sizes
    T, D = xv.shape
    C = cxv.shape[0]
    samples = condv.shape[0]
    cols = owv.shape[1]
    width = qwv.shape[1]
    heads = width // HEAD
    blocks = T // REACH
    sp, tp, dp = lax.axis_index("sp"), lax.axis_index("tp"), lax.axis_index("dp")

    def z_at(d):
        return {"sp": lax.rem(sp + d + SP, SP)}

    barrier = pltpu.get_barrier_semaphore()
    z_far = sorted(range(1, SP), key=lambda d: -min(d, SP - d))
    xy_off = [(t, d) for t in range(TP) for d in range(DP) if (t, d) != (0, 0)]
    for d in z_far:
        pl.semaphore_signal(barrier, inc=1, device_id=z_at(d), device_id_type=MESH)
    for t, d in xy_off:
        pl.semaphore_signal(
            barrier, inc=1, device_id={"tp": lax.rem(tp + t, TP), "dp": lax.rem(dp + d, DP)}, device_id_type=MESH
        )

    pairs = [(cond, condv), (cctx, cctxv), (mod, modv), (lat, xv), (ctx, cxv), (kw, kvw.at[0:HEAD]),
             (vw, kvw.at[HEAD:LANES]), (qw, qwv), (ow, owv), (sink, sinks), (bias, biass)]
    loads = []
    for i, (src, dst) in enumerate(pairs):
        copy = pltpu.make_async_copy(src, dst, in_sems.at[i])
        copy.start()
        loads.append(copy)

    loads[0].wait()
    loads[1].wait()
    loads[2].wait()
    act = jax.nn.silu(condv[...].astype(F32)).astype(BF16)
    act_c = jax.nn.silu(jnp.broadcast_to(cctxv[...].astype(F32), (8, cctxv.shape[1]))).astype(BF16)
    half = samples // 2
    weights = modv[...].reshape(-1, modv.shape[2])
    rows = dot_t(act, weights)
    side = dot_t(act_c, weights[0:LANES])
    zsend[...] = rows[:, 0:LANES]
    zcsend[...] = side[0:1]
    gsend[...] = jnp.concatenate([rows[:half, LANES:], rows[half:, LANES:]], axis=1)

    def norm_rows(src, dst, rows):
        def step(i, _):
            r = pl.ds(pl.multiple_of(i * rows, rows), rows)
            v = src[r, :].astype(F32)
            v = v - jnp.mean(v, axis=-1, keepdims=True)
            dst[r, :] = v * lax.rsqrt(jnp.mean(v * v, axis=-1, keepdims=True) + EPS)
            return 0

        lax.fori_loop(0, src.shape[0] // rows, step, 0)

    pl.semaphore_wait(barrier, len(z_far) + len(xy_off))
    for src, dst, i in ((zcsend, zcrecv, 1), (zsend, zrecv, 0)):
        for d in z_far:
            pltpu.make_async_remote_copy(
                src_ref=src, dst_ref=dst.at[d - 1], send_sem=z_send.at[i], recv_sem=z_recv.at[i],
                device_id=z_at(d), device_id_type=MESH,
            ).start()

    loads[3].wait()
    norm_rows(xv, xn, REACH)
    loads[4].wait()
    norm_rows(cxv, cxn, C)
    kvc[:, LANES:] = jnp.ones((kvc.shape[0], LANES), BF16)
    kvx[:, LANES:] = jnp.ones((kvx.shape[0], LANES), BF16)

    lane = lane_iota((T, LANES))
    pos = lax.broadcasted_iota(jnp.int32, (T, LANES), 0) + sp * T
    inner = lane & 31
    freq = jnp.exp((inner & 15).astype(F32) * (-2.0 / 32.0 * math.log(BASE)))
    place = jnp.where((lane & 63) < 32, pos >> 6, pos & 63).astype(F32)
    angle = place * freq
    ct[...] = jnp.cos(angle)
    sine = jnp.sin(angle)
    st[...] = jnp.where(inner < 16, -sine, sine)
    loads[5].wait()
    loads[6].wait()

    pltpu.make_async_copy(zcrecv, zcrecv, z_recv.at[1]).wait()
    pltpu.make_async_copy(zrecv, zrecv, z_recv.at[0]).wait()
    total = zsend[...]
    total_c = zcsend[...]
    for d in range(SP - 1):
        total = total + zrecv[d]
        total_c = total_c + zcrecv[d]
    for s in range(samples):
        xysend[s, 0:1, :] = total[s:s + 1]
        xysend[s, 1:2, :] = total_c[0:1]
    me = tp * DP + dp
    for t, d in sorted(xy_off, key=lambda o: -(min(o[0], TP - o[0]) + min(o[1], DP - o[1]) // 2)):
        target = lax.rem(dp + d, DP)
        pltpu.make_async_remote_copy(
            src_ref=xysend.at[target], dst_ref=xyrecv.at[me], send_sem=xy_send, recv_sem=xy_recv,
            device_id={"tp": lax.rem(tp + t, TP), "dp": target}, device_id_type=MESH,
        ).start()
    xyrecv[me] = xysend[dp]
    for d in z_far:
        pltpu.make_async_remote_copy(
            src_ref=gsend, dst_ref=grecv.at[d - 1], send_sem=g_sems.at[0], recv_sem=g_sems.at[1],
            device_id=z_at(d), device_id_type=MESH,
        ).start()
    others = xyrecv.at[pl.ds(0, len(xy_off))]
    pltpu.make_async_copy(others, others, xy_recv).wait()
    chunks = vecs.shape[1]
    low2 = lane_iota((2, LANES)) < 64
    for k in range(chunks):
        left, right = xyrecv[2 * k], xyrecv[2 * k + 1]
        vecs[0, k] = jnp.where(low2, left, pltpu.roll(right, 64, 1))
        vecs[1, k] = jnp.where(low2, pltpu.roll(left, 64, 1), right) + 1.0

    def ctx_at(d, count=1):
        return kvc.at[pl.ds(SLOT[d] * C, count * C), pl.ds(0, LANES)]

    def ctx_copy(slot_from, slot_to, d, sem):
        return pltpu.make_async_remote_copy(
            src_ref=ctx_at(slot_from), dst_ref=ctx_at(slot_to), send_sem=c_send, recv_sem=c_recv.at[sem],
            device_id=z_at(d), device_id_type=MESH,
        )

    for k in range(chunks):
        c = slice(k * LANES, (k + 1) * LANES)
        cxb[:, c] = (cxn[:, c] * vecs[1, k, 1:2, :] + vecs[0, k, 1:2, :]).astype(BF16)
    kvc[0:C, 0:LANES] = dot_t(cxb[...], kvw[...]).astype(BF16)
    for d in DIRECT:
        ctx_copy(0, d, d, {5: 1, -5: 2}.get(d, 0)).start()

    def modulate(k, _):
        c = pl.ds(pl.multiple_of(k * LANES, LANES), LANES)
        xb[:, c] = (xn[:, c] * vecs[1, k, 0:1, :] + vecs[0, k, 0:1, :]).astype(BF16)
        return 0

    lax.fori_loop(0, chunks, modulate, 0)

    def partner(v):
        low = (lane_iota(v.shape) & 31) < 16
        return jnp.where(low, pltpu.roll(v, LANES - 16, 1), pltpu.roll(v, 16, 1))

    kv = dot_t(xb[...], kvw[...])
    is_key = lane_iota((T, LANES)) < 64
    kv = jnp.where(is_key, kv * ct[...] + partner(kv) * st[...], kv)
    kvx[REACH:REACH + T, 0:LANES] = kv.astype(BF16)
    sends = []
    for side_index, (at, to, there_at) in enumerate(((T, 1, 0), (REACH, -1, REACH + T))):
        copy = pltpu.make_async_remote_copy(
            src_ref=kvx.at[pl.ds(at, REACH), pl.ds(0, LANES)], dst_ref=kvx.at[pl.ds(there_at, REACH), pl.ds(0, LANES)],
            send_sem=h_send, recv_sem=h_recv.at[side_index], device_id=z_at(to), device_id_type=MESH,
        )
        copy.start()
        sends.append(copy)

    loads[7].wait()
    factor = LOG2E * HEAD ** (-0.5)
    low_lane = lane_iota((T, LANES)) < 64
    for j in range(width // LANES):
        q = dot(xb[...], qwv[:, j * LANES:(j + 1) * LANES])
        q = (q * ct[...] + partner(q) * st[...]) * factor
        qz[2 * j] = jnp.where(low_lane, q, 0.0).astype(BF16)
        qz[2 * j + 1] = jnp.where(low_lane, pltpu.roll(q, 64, 1), 0.0).astype(BF16)

    loads[9].wait()
    loads[10].wait()

    def per_head(ref, count):
        return jnp.concatenate([jnp.full((count, LANES), ref[h] * LOG2E, F32) for h in range(heads)], axis=0)

    def of_rows(ref, start, count):
        return ref[:, start:start + count, :].reshape(heads * count, ref.shape[2])

    def keep_state(start, count, m, acc):
        mw[:, start:start + count, :] = m.reshape(heads, count, LANES)
        accw[:, start:start + count, :] = acc.reshape(heads, count, 2 * LANES)

    def window(b):
        keys = kvx[b * REACH:(b + 3) * REACH, :]
        s = dot_t(of_rows(qz, b * REACH, REACH), keys[:, 0:LANES])
        i = lax.broadcasted_iota(jnp.int32, (REACH, 3 * REACH), 0)
        j = lax.broadcasted_iota(jnp.int32, (REACH, 3 * REACH), 1)
        valid = (j >= i) & (j <= i + 2 * REACH)
        if b == 0:
            valid = valid & (sp * T - REACH + j >= 0)
        if b == blocks - 1:
            valid = valid & (sp * T + (b - 1) * REACH + j < SP * T)
        s = jnp.where(valid[None], s.reshape(heads, REACH, 3 * REACH), MASKED).reshape(heads * REACH, 3 * REACH)
        m = full(jnp.max(s, axis=1, keepdims=True))
        keep_state(b * REACH, REACH, m, dot(jnp.exp2(s - wide(m, 3 * REACH)).astype(BF16), keys))

    def arrived(d, count, sem):
        blocks_here = ctx_at(d, count)
        pltpu.make_async_copy(blocks_here, blocks_here, c_recv.at[sem]).wait()

    def context(start, count, keys, others):
        s = dot_t(of_rows(qz, start, count), keys[:, 0:LANES])
        bias2 = per_head(biass, count)
        m0 = of_rows(mw, start, count)
        m = jnp.maximum(m0, full(jnp.max(s, axis=1, keepdims=True)) + bias2)
        if others is not None:
            m = jnp.maximum(m, others)
        p = jnp.exp2(s - wide(m - bias2, keys.shape[0])).astype(BF16)
        return m, dot(p, keys) + of_rows(accw, start, count) * wide(jnp.exp2(m0 - m), 2 * LANES)

    soon, late = SLOT[SOON[0]] * C, SLOT[LATE[0]] * C

    pltpu.make_async_copy(grecv, grecv, g_sems.at[1]).wait()
    gates = gsend[...]
    for d in range(SP - 1):
        gates = gates + grecv[d]
    gsum[...] = gates
    ghave[dp] = gates
    for d in range(1, DP):
        pltpu.make_async_remote_copy(
            src_ref=gsum, dst_ref=ghave.at[dp], send_sem=g_sems.at[2], recv_sem=g_sems.at[3],
            device_id={"dp": lax.rem(dp + d, DP)}, device_id_type=MESH,
        ).start()
    for b in range(1, blocks - 1):
        window(b)
    arrived(5, 1, 1)
    for slot_to, d in ((8, 3), (7, 2), (3, -2), (6, 1), (4, -1)):
        ctx_copy(5, slot_to, d, 4 if slot_to in LATE else 3).start()
    arrived(-5, 1, 2)
    for slot_to, d in ((-7, -2), (-6, -1), (-4, 1)):
        ctx_copy(-5, slot_to, d, 4 if slot_to in LATE else 3).start()
    for copy in sends:
        copy.wait_recv()
    arrived(NEAR[0], len(NEAR), 0)
    for b in (0, blocks - 1):
        window(b)
    for b in range(blocks):
        keep_state(b * REACH, REACH, *context(b * REACH, REACH, kvc[0:soon, :], None))
    arrived(SOON[0], len(SOON), 3)
    for b in range(blocks):
        keep_state(b * REACH, REACH, *context(b * REACH, REACH, kvc[soon:late, :], None))
    arrived(LATE[0], len(LATE), 4)

    def tp_copy(i, way):
        up = way in (0, 2)
        owner = tp if way < 2 else lax.rem(tp + (TP - 1 if up else 1), TP)
        rows = pl.ds(i * PIECE + (PIECE // 2 if way == 3 else 0), PIECE // 2 if way >= 2 else PIECE)
        return pltpu.make_async_remote_copy(
            src_ref=gath.at[owner, rows], dst_ref=gath.at[owner, rows], send_sem=y_send,
            recv_sem=y_recv.at[i, way], device_id={"tp": lax.rem(tp + (1 if up else TP - 1), TP)}, device_id_type=MESH,
        )

    pieces = T // PIECE
    sink2 = per_head(sinks, REACH)
    low = lane_iota((REACH, LANES)) < 64
    for b in range(blocks):
        m, acc = context(b * REACH, REACH, kvc[late:, :], sink2)
        att = acc[:, 0:LANES] / (acc[:, LANES:] + jnp.exp2(sink2 - m))
        att = att.reshape(heads, REACH, LANES)
        for j in range(heads // 2):
            pair = jnp.where(low, pltpu.roll(att[2 * j], 64, 1), att[2 * j + 1])
            gath[tp, b * REACH:(b + 1) * REACH, j * LANES:(j + 1) * LANES] = pair.astype(BF16)
        for i in range(b * REACH // PIECE, (b + 1) * REACH // PIECE):
            tp_copy(i, 0).start()
            tp_copy(i, 1).start()

    loads[8].wait()

    def projected(owner, rows):
        return dot(gath[owner, rows, :], owv[pl.ds(pl.multiple_of(owner * width, width), width), :])

    above, below, opposite = (lax.rem(tp + t, TP) for t in (1, TP - 1, 2))
    mixed[...] = projected(tp, pl.ds(0, T))
    for b in range(blocks):
        for i in range(b * REACH // PIECE, (b + 1) * REACH // PIECE):
            for way in (0, 1):
                tp_copy(i, way).wait_recv()
                tp_copy(i, way + 2).start()
        rows = pl.ds(b * REACH, REACH)
        mixed[rows, :] = mixed[rows, :] + projected(above, rows) + projected(below, rows)

    others = ghave.at[pl.ds(0, DP - 1)]
    pltpu.make_async_copy(others, others, g_sems.at[3]).wait()
    low1 = lane_iota((1, LANES)) < 64
    gate_chunks = []
    for k in range(DP // 2):
        left, right = (ghave[2 * k + i, pl.ds(lax.rem(dp, half), 1), :] for i in range(2))
        gate_chunks.append(jnp.where(
            dp < half,
            jnp.where(low1, left, pltpu.roll(right, 64, 1)),
            jnp.where(low1, pltpu.roll(left, 64, 1), right),
        ))
    gate = jnp.concatenate(gate_chunks, axis=1)
    for b in range(blocks):
        rows = pl.ds(b * REACH, REACH)
        for i in range(b * REACH // PIECE, (b + 1) * REACH // PIECE):
            tp_copy(i, 2).wait_recv()
            tp_copy(i, 3).wait_recv()
        own = xv[rows, pl.ds(pl.multiple_of(tp * cols, LANES), cols)].astype(F32)
        out[rows, :] = own + gate * (mixed[rows, :] + projected(opposite, rows))

    others = gath.at[pl.ds(0, TP - 1)]
    pltpu.make_async_copy(others, others, y_send).wait()
    others = kvx.at[pl.ds(0, 2 * REACH), pl.ds(0, LANES)]
    pltpu.make_async_copy(others, others, h_send).wait()
    pltpu.make_async_copy(zrecv, zrecv, z_send.at[0]).wait()
    pltpu.make_async_copy(zcrecv, zcrecv, z_send.at[1]).wait()
    pltpu.make_async_copy(grecv, grecv, g_sems.at[0]).wait()
    others = ghave.at[pl.ds(0, DP - 1)]
    pltpu.make_async_copy(others, others, g_sems.at[2]).wait()
    others = xyrecv.at[pl.ds(0, len(xy_off))]
    pltpu.make_async_copy(others, others, xy_send).wait()
    others = kvc.at[pl.ds(C, (SP - 1) * C), pl.ds(0, LANES)]
    pltpu.make_async_copy(others, others, c_send).wait()


def per_device(sizes, lat, cond, cctx, mod, ctx, qw, kw, vw, ow, sink, bias):
    SP, TP, DP = sizes
    T, D = lat.shape[1:]
    C = ctx.shape[1]
    width = qw.shape[1]
    heads = width // HEAD
    blocks = T // REACH
    cols = ow.shape[1]
    samples = cond.shape[0]
    any_space = pl.BlockSpec(memory_space=pl.ANY)
    vmem = pltpu.VMEM
    dma = pltpu.SemaphoreType.DMA
    scratch = [
        vmem((T, D), BF16), vmem(cond.shape, BF16), vmem((1, cctx.shape[0]), BF16), vmem((mod.shape[0], mod.shape[2], mod.shape[1]), BF16),
        vmem((C, D), BF16), vmem(qw.shape, BF16), vmem(ow.shape, BF16),
        pltpu.SMEM(sink.shape, F32), pltpu.SMEM(bias.shape, F32),
        vmem((samples, LANES), F32), vmem((1, LANES), F32), vmem((SP - 1, samples, LANES), F32), vmem((SP - 1, 1, LANES), F32),
        vmem((samples // 2, LANES), F32), vmem((SP - 1, samples // 2, LANES), F32), vmem((samples // 2, LANES), F32),
        vmem((DP, samples // 2, LANES), F32),
        vmem((samples, 2, LANES), F32), vmem((TP * DP, 2, LANES), F32), vmem((2, TP * DP // 2, 2, LANES), F32),
        vmem((T, D), F32), vmem((C, D), F32), vmem((T, D), BF16), vmem((C, D), BF16), vmem((LANES, D), BF16),
        vmem((T, LANES), F32), vmem((T, LANES), F32),
        vmem((SP * C, 2 * LANES), BF16), vmem((T + 2 * REACH, 2 * LANES), BF16), vmem((heads, T, LANES), BF16),
        vmem((heads, T, 2 * LANES), F32), vmem((heads, T, LANES), F32),
        vmem((TP, T, width), BF16), vmem((T, cols), F32),
        dma((11,)),
        dma((2,)), dma((2,)), dma, dma, dma, dma((5,)), dma, dma((2,)), dma, dma((T // PIECE, 4)), dma((4,)),
    ]
    result = pl.pallas_call(
        functools.partial(kernel, sizes),
        out_shape=vmem((T, cols), F32),
        in_specs=[any_space] * 11,
        out_specs=pl.BlockSpec(memory_space=vmem),
        scratch_shapes=scratch,
        compiler_params=pltpu.CompilerParams(
            collective_id=0, has_side_effects=True, vmem_limit_bytes=48 * 1024 * 1024
        ),
        name="step",
    )(*(pltpu.with_memory_space_constraint(v, pltpu.HBM) for v in (
        lat[0], cond, cctx[None, :], mod.transpose(0, 2, 1), ctx[0], qw, kw.T, vw.T, ow, sink, bias
    )))
    return result[None]


def solution(mesh):
    placed = (
        P("dp", "sp", None),
        P(None, "sp"),
        P("sp"),
        P(None, "sp", ("tp", "dp")),
        P("dp", "sp", None),
        P(None, "tp"),
        P(None, "tp"),
        P(None, "tp"),
        P(None, "tp"),
        P("tp"),
        P("tp"),
    )
    sizes = (mesh.shape["sp"], mesh.shape["tp"], mesh.shape["dp"])
    return jax.shard_map(
        functools.partial(per_device, sizes),
        mesh=mesh, in_specs=placed, out_specs=P("dp", "sp", "tp"), check_vma=False,
    )
```

```python
import functools
import math

import jax
import jax.numpy as jnp
from jax import lax
from jax.experimental import pallas as pl
from jax.experimental.pallas import tpu as pltpu
from jax.sharding import PartitionSpec as P

HEAD = 64
GRID_W = 64
REACH = 128
EPS = 1e-06
BASE = 10000.0
MASKED = -1e30
LOG2E = math.log2(math.e)
F32 = jnp.float32
BF16 = jnp.bfloat16
LANES = 128
MESH = pl.DeviceIdType.MESH


def dot(a, b):
    return jnp.dot(a, b, preferred_element_type=F32)


def dot_t(a, b):
    return lax.dot_general(a, b, (((1,), (1,)), ((), ())), preferred_element_type=F32)


def full(v):
    return jnp.broadcast_to(v, (v.shape[0], LANES))


def wide(v, width):
    return jnp.concatenate([v] * (width // LANES), axis=1)


def lane_iota(shape):
    return lax.broadcasted_iota(jnp.int32, shape, len(shape) - 1)


DIRECT = (5, -5, 1, -1, 2, -2, -3)
NEAR = (1, -1, 2, -2, -3)
SOON = (4, 6, -4, -6)
LATE = (3, 7, 8, -7)
SLOT = {d: i for i, d in enumerate((0, *NEAR, 5, -5, *SOON, *LATE))}
PIECE = 64


def kernel(
    sizes,
    lat, cond, cctx, mod, ctx, qw, kw, vw, ow, sink, bias,
    out,
    xv, condv, cctxv, modv, cxv, qwv, owv, sinks, biass,
    zsend, zcsend, zrecv, zcrecv, gsend, grecv, gsum, ghave, xysend, xyrecv, xycsend, xycrecv, vecs,
    xn, cxn, xb, cxb, kvw, ct, st,
    kvc, kvx, qz, accw, mw, gath, mixed,
    in_sems,
    z_send, z_recv, xy_send, xy_recv, c_send, c_recv, h_send, h_recv, y_send, y_recv, g_sems,
):
    SP, TP, DP = sizes
    T, D = xv.shape
    C = cxv.shape[0]
    samples = condv.shape[0]
    cols = owv.shape[1]
    width = qwv.shape[1]
    heads = width // HEAD
    blocks = T // REACH
    sp, tp, dp = lax.axis_index("sp"), lax.axis_index("tp"), lax.axis_index("dp")

    def z_at(d):
        return {"sp": lax.rem(sp + d + SP, SP)}

    barrier = pltpu.get_barrier_semaphore()
    z_far = sorted(range(1, SP), key=lambda d: -min(d, SP - d))
    xy_off = [(t, d) for t in range(TP) for d in range(DP) if (t, d) != (0, 0)]
    for d in z_far:
        pl.semaphore_signal(barrier, inc=1, device_id=z_at(d), device_id_type=MESH)
    for t, d in xy_off:
        pl.semaphore_signal(
            barrier, inc=1, device_id={"tp": lax.rem(tp + t, TP), "dp": lax.rem(dp + d, DP)}, device_id_type=MESH
        )

    pairs = [(cond, condv), (cctx, cctxv), (mod, modv), (lat, xv), (ctx, cxv), (kw, kvw.at[0:HEAD]),
             (vw, kvw.at[HEAD:LANES]), (qw, qwv), (ow, owv), (sink, sinks), (bias, biass)]
    loads = []
    for i, (src, dst) in enumerate(pairs):
        copy = pltpu.make_async_copy(src, dst, in_sems.at[i])
        copy.start()
        loads.append(copy)

    loads[0].wait()
    loads[1].wait()
    loads[2].wait()
    act = jax.nn.silu(condv[...].astype(F32)).astype(BF16)
    act_c = jax.nn.silu(jnp.broadcast_to(cctxv[...].astype(F32), (8, cctxv.shape[1]))).astype(BF16)
    half = samples // 2
    weights = modv[...].reshape(-1, modv.shape[2])
    rows = dot_t(act, weights)
    side = dot_t(act_c, weights[0:LANES])
    zsend[...] = rows[:, 0:LANES]
    zcsend[...] = side[0:1]
    gsend[...] = jnp.concatenate([rows[:half, LANES:], rows[half:, LANES:]], axis=1)

    def norm_rows(src, dst, rows):
        def step(i, _):
            r = pl.ds(pl.multiple_of(i * rows, rows), rows)
            v = src[r, :].astype(F32)
            v = v - jnp.mean(v, axis=-1, keepdims=True)
            dst[r, :] = v * lax.rsqrt(jnp.mean(v * v, axis=-1, keepdims=True) + EPS)
            return 0

        lax.fori_loop(0, src.shape[0] // rows, step, 0)

    pl.semaphore_wait(barrier, len(z_far) + len(xy_off))
    for src, dst, i in ((zcsend, zcrecv, 1), (zsend, zrecv, 0)):
        for d in z_far:
            pltpu.make_async_remote_copy(
                src_ref=src, dst_ref=dst.at[d - 1], send_sem=z_send.at[i], recv_sem=z_recv.at[i],
                device_id=z_at(d), device_id_type=MESH,
            ).start()

    loads[3].wait()
    norm_rows(xv, xn, REACH)
    loads[4].wait()
    norm_rows(cxv, cxn, C)
    kvc[:, LANES:] = jnp.ones((kvc.shape[0], LANES), BF16)
    kvx[:, LANES:] = jnp.ones((kvx.shape[0], LANES), BF16)

    lane = lane_iota((T, LANES))
    pos = lax.broadcasted_iota(jnp.int32, (T, LANES), 0) + sp * T
    inner = lane & 31
    freq = jnp.exp((inner & 15).astype(F32) * (-2.0 / 32.0 * math.log(BASE)))
    place = jnp.where((lane & 63) < 32, pos >> 6, pos & 63).astype(F32)
    angle = place * freq
    ct[...] = jnp.cos(angle)
    sine = jnp.sin(angle)
    st[...] = jnp.where(inner < 16, -sine, sine)
    loads[5].wait()
    loads[6].wait()

    me = tp * DP + dp
    xy_order = sorted(xy_off, key=lambda o: -(min(o[0], TP - o[0]) + min(o[1], DP - o[1]) // 2))

    def xy_copy(src, dst, t, target, i):
        return pltpu.make_async_remote_copy(
            src_ref=src, dst_ref=dst.at[me], send_sem=xy_send.at[i], recv_sem=xy_recv.at[i],
            device_id={"tp": lax.rem(tp + t, TP), "dp": target}, device_id_type=MESH,
        )

    pltpu.make_async_copy(zcrecv, zcrecv, z_recv.at[1]).wait()
    total_c = zcsend[...]
    for d in range(SP - 1):
        total_c = total_c + zcrecv[d]
    xycsend[...] = total_c
    for t, d in xy_order:
        xy_copy(xycsend, xycrecv, t, lax.rem(dp + d, DP), 1).start()
    xycrecv[me] = total_c
    pltpu.make_async_copy(zrecv, zrecv, z_recv.at[0]).wait()
    total = zsend[...]
    for d in range(SP - 1):
        total = total + zrecv[d]
    for s in range(samples):
        xysend[s] = total[s:s + 1]
    for t, d in xy_order:
        target = lax.rem(dp + d, DP)
        xy_copy(xysend.at[target], xyrecv, t, target, 0).start()
    xyrecv[me] = xysend[dp]
    for d in z_far:
        pltpu.make_async_remote_copy(
            src_ref=gsend, dst_ref=grecv.at[d - 1], send_sem=g_sems.at[0], recv_sem=g_sems.at[1],
            device_id=z_at(d), device_id_type=MESH,
        ).start()
    chunks = vecs.shape[2]
    low1 = lane_iota((1, LANES)) < 64

    def vectors(which, got, i):
        others = got.at[pl.ds(0, len(xy_off))]
        pltpu.make_async_copy(others, others, xy_recv.at[i]).wait()
        for k in range(chunks):
            left, right = got[2 * k], got[2 * k + 1]
            vecs[which, 0, k] = jnp.where(low1, left, pltpu.roll(right, 64, 1))
            vecs[which, 1, k] = jnp.where(low1, pltpu.roll(left, 64, 1), right) + 1.0

    vectors(1, xycrecv, 1)

    def ctx_at(d, count=1):
        return kvc.at[pl.ds(SLOT[d] * C, count * C), pl.ds(0, LANES)]

    def ctx_copy(slot_from, slot_to, d, sem):
        return pltpu.make_async_remote_copy(
            src_ref=ctx_at(slot_from), dst_ref=ctx_at(slot_to), send_sem=c_send, recv_sem=c_recv.at[sem],
            device_id=z_at(d), device_id_type=MESH,
        )

    for k in range(chunks):
        c = slice(k * LANES, (k + 1) * LANES)
        cxb[:, c] = (cxn[:, c] * vecs[1, 1, k] + vecs[1, 0, k]).astype(BF16)
    kvc[0:C, 0:LANES] = dot_t(cxb[...], kvw[...]).astype(BF16)
    for d in DIRECT:
        ctx_copy(0, d, d, {5: 1, -5: 2}.get(d, 0)).start()

    vectors(0, xyrecv, 0)
    def modulate(k, _):
        c = pl.ds(pl.multiple_of(k * LANES, LANES), LANES)
        xb[:, c] = (xn[:, c] * vecs[0, 1, k] + vecs[0, 0, k]).astype(BF16)
        return 0

    lax.fori_loop(0, chunks, modulate, 0)

    def partner(v):
        low = (lane_iota(v.shape) & 31) < 16
        return jnp.where(low, pltpu.roll(v, LANES - 16, 1), pltpu.roll(v, 16, 1))

    kv = dot_t(xb[...], kvw[...])
    is_key = lane_iota((T, LANES)) < 64
    kv = jnp.where(is_key, kv * ct[...] + partner(kv) * st[...], kv)
    kvx[REACH:REACH + T, 0:LANES] = kv.astype(BF16)
    sends = []
    for side_index, (at, to, there_at) in enumerate(((T, 1, 0), (REACH, -1, REACH + T))):
        copy = pltpu.make_async_remote_copy(
            src_ref=kvx.at[pl.ds(at, REACH), pl.ds(0, LANES)], dst_ref=kvx.at[pl.ds(there_at, REACH), pl.ds(0, LANES)],
            send_sem=h_send, recv_sem=h_recv.at[side_index], device_id=z_at(to), device_id_type=MESH,
        )
        copy.start()
        sends.append(copy)

    loads[7].wait()
    factor = LOG2E * HEAD ** (-0.5)
    low_lane = lane_iota((T, LANES)) < 64
    for j in range(width // LANES):
        q = dot(xb[...], qwv[:, j * LANES:(j + 1) * LANES])
        q = (q * ct[...] + partner(q) * st[...]) * factor
        qz[2 * j] = jnp.where(low_lane, q, 0.0).astype(BF16)
        qz[2 * j + 1] = jnp.where(low_lane, pltpu.roll(q, 64, 1), 0.0).astype(BF16)

    loads[9].wait()
    loads[10].wait()

    def per_head(ref, count):
        return jnp.concatenate([jnp.full((count, LANES), ref[h] * LOG2E, F32) for h in range(heads)], axis=0)

    def of_rows(ref, start, count):
        return ref[:, start:start + count, :].reshape(heads * count, ref.shape[2])

    def keep_state(start, count, m, acc):
        mw[:, start:start + count, :] = m.reshape(heads, count, LANES)
        accw[:, start:start + count, :] = acc.reshape(heads, count, 2 * LANES)

    def window(b):
        keys = kvx[b * REACH:(b + 3) * REACH, :]
        s = dot_t(of_rows(qz, b * REACH, REACH), keys[:, 0:LANES])
        i = lax.broadcasted_iota(jnp.int32, (REACH, 3 * REACH), 0)
        j = lax.broadcasted_iota(jnp.int32, (REACH, 3 * REACH), 1)
        valid = (j >= i) & (j <= i + 2 * REACH)
        if b == 0:
            valid = valid & (sp * T - REACH + j >= 0)
        if b == blocks - 1:
            valid = valid & (sp * T + (b - 1) * REACH + j < SP * T)
        s = jnp.where(valid[None], s.reshape(heads, REACH, 3 * REACH), MASKED).reshape(heads * REACH, 3 * REACH)
        m = full(jnp.max(s, axis=1, keepdims=True))
        keep_state(b * REACH, REACH, m, dot(jnp.exp2(s - wide(m, 3 * REACH)).astype(BF16), keys))

    def arrived(d, count, sem):
        blocks_here = ctx_at(d, count)
        pltpu.make_async_copy(blocks_here, blocks_here, c_recv.at[sem]).wait()

    def context(start, count, keys, others):
        s = dot_t(of_rows(qz, start, count), keys[:, 0:LANES])
        bias2 = per_head(biass, count)
        m0 = of_rows(mw, start, count)
        m = jnp.maximum(m0, full(jnp.max(s, axis=1, keepdims=True)) + bias2)
        if others is not None:
            m = jnp.maximum(m, others)
        p = jnp.exp2(s - wide(m - bias2, keys.shape[0])).astype(BF16)
        return m, dot(p, keys) + of_rows(accw, start, count) * wide(jnp.exp2(m0 - m), 2 * LANES)

    soon, late = SLOT[SOON[0]] * C, SLOT[LATE[0]] * C

    pltpu.make_async_copy(grecv, grecv, g_sems.at[1]).wait()
    gates = gsend[...]
    for d in range(SP - 1):
        gates = gates + grecv[d]
    gsum[...] = gates
    ghave[dp] = gates
    for d in range(1, DP):
        pltpu.make_async_remote_copy(
            src_ref=gsum, dst_ref=ghave.at[dp], send_sem=g_sems.at[2], recv_sem=g_sems.at[3],
            device_id={"dp": lax.rem(dp + d, DP)}, device_id_type=MESH,
        ).start()
    for b in range(1, blocks - 1):
        window(b)
    arrived(5, 1, 1)
    for slot_to, d in ((8, 3), (7, 2), (3, -2), (6, 1), (4, -1)):
        ctx_copy(5, slot_to, d, 4 if slot_to in LATE else 3).start()
    arrived(-5, 1, 2)
    for slot_to, d in ((-7, -2), (-6, -1), (-4, 1)):
        ctx_copy(-5, slot_to, d, 4 if slot_to in LATE else 3).start()
    for copy in sends:
        copy.wait_recv()
    arrived(NEAR[0], len(NEAR), 0)
    for b in (0, blocks - 1):
        window(b)
    for b in range(blocks):
        keep_state(b * REACH, REACH, *context(b * REACH, REACH, kvc[0:soon, :], None))
    arrived(SOON[0], len(SOON), 3)
    for b in range(blocks):
        keep_state(b * REACH, REACH, *context(b * REACH, REACH, kvc[soon:late, :], None))
    arrived(LATE[0], len(LATE), 4)

    def tp_copy(i, way):
        up = way in (0, 2)
        owner = tp if way < 2 else lax.rem(tp + (TP - 1 if up else 1), TP)
        rows = pl.ds(i * PIECE + (PIECE // 2 if way == 3 else 0), PIECE // 2 if way >= 2 else PIECE)
        return pltpu.make_async_remote_copy(
            src_ref=gath.at[owner, rows], dst_ref=gath.at[owner, rows], send_sem=y_send,
            recv_sem=y_recv.at[i, way], device_id={"tp": lax.rem(tp + (1 if up else TP - 1), TP)}, device_id_type=MESH,
        )

    pieces = T // PIECE
    sink2 = per_head(sinks, REACH)
    low = lane_iota((REACH, LANES)) < 64
    for b in range(blocks):
        m, acc = context(b * REACH, REACH, kvc[late:, :], sink2)
        att = acc[:, 0:LANES] / (acc[:, LANES:] + jnp.exp2(sink2 - m))
        att = att.reshape(heads, REACH, LANES)
        for j in range(heads // 2):
            pair = jnp.where(low, pltpu.roll(att[2 * j], 64, 1), att[2 * j + 1])
            gath[tp, b * REACH:(b + 1) * REACH, j * LANES:(j + 1) * LANES] = pair.astype(BF16)
        for i in range(b * REACH // PIECE, (b + 1) * REACH // PIECE):
            tp_copy(i, 0).start()
            tp_copy(i, 1).start()

    loads[8].wait()

    def projected(owner, rows):
        return dot(gath[owner, rows, :], owv[pl.ds(pl.multiple_of(owner * width, width), width), :])

    above, below, opposite = (lax.rem(tp + t, TP) for t in (1, TP - 1, 2))
    mixed[...] = projected(tp, pl.ds(0, T))
    for b in range(blocks):
        for i in range(b * REACH // PIECE, (b + 1) * REACH // PIECE):
            for way in (0, 1):
                tp_copy(i, way).wait_recv()
                tp_copy(i, way + 2).start()
        rows = pl.ds(b * REACH, REACH)
        mixed[rows, :] = mixed[rows, :] + projected(above, rows) + projected(below, rows)

    others = ghave.at[pl.ds(0, DP - 1)]
    pltpu.make_async_copy(others, others, g_sems.at[3]).wait()
    gate_chunks = []
    for k in range(DP // 2):
        left, right = (ghave[2 * k + i, pl.ds(lax.rem(dp, half), 1), :] for i in range(2))
        gate_chunks.append(jnp.where(
            dp < half,
            jnp.where(low1, left, pltpu.roll(right, 64, 1)),
            jnp.where(low1, pltpu.roll(left, 64, 1), right),
        ))
    gate = jnp.concatenate(gate_chunks, axis=1)
    for b in range(blocks):
        rows = pl.ds(b * REACH, REACH)
        for i in range(b * REACH // PIECE, (b + 1) * REACH // PIECE):
            tp_copy(i, 2).wait_recv()
            tp_copy(i, 3).wait_recv()
        own = xv[rows, pl.ds(pl.multiple_of(tp * cols, LANES), cols)].astype(F32)
        out[rows, :] = own + gate * (mixed[rows, :] + projected(opposite, rows))

    others = gath.at[pl.ds(0, TP - 1)]
    pltpu.make_async_copy(others, others, y_send).wait()
    others = kvx.at[pl.ds(0, 2 * REACH), pl.ds(0, LANES)]
    pltpu.make_async_copy(others, others, h_send).wait()
    pltpu.make_async_copy(zrecv, zrecv, z_send.at[0]).wait()
    pltpu.make_async_copy(zcrecv, zcrecv, z_send.at[1]).wait()
    pltpu.make_async_copy(grecv, grecv, g_sems.at[0]).wait()
    others = ghave.at[pl.ds(0, DP - 1)]
    pltpu.make_async_copy(others, others, g_sems.at[2]).wait()
    for i in range(2):
        others = xyrecv.at[pl.ds(0, len(xy_off))]
        pltpu.make_async_copy(others, others, xy_send.at[i]).wait()
    others = kvc.at[pl.ds(C, (SP - 1) * C), pl.ds(0, LANES)]
    pltpu.make_async_copy(others, others, c_send).wait()


def per_device(sizes, lat, cond, cctx, mod, ctx, qw, kw, vw, ow, sink, bias):
    SP, TP, DP = sizes
    T, D = lat.shape[1:]
    C = ctx.shape[1]
    width = qw.shape[1]
    heads = width // HEAD
    blocks = T // REACH
    cols = ow.shape[1]
    samples = cond.shape[0]
    any_space = pl.BlockSpec(memory_space=pl.ANY)
    vmem = pltpu.VMEM
    dma = pltpu.SemaphoreType.DMA
    scratch = [
        vmem((T, D), BF16), vmem(cond.shape, BF16), vmem((1, cctx.shape[0]), BF16), vmem((mod.shape[0], mod.shape[2], mod.shape[1]), BF16),
        vmem((C, D), BF16), vmem(qw.shape, BF16), vmem(ow.shape, BF16),
        pltpu.SMEM(sink.shape, F32), pltpu.SMEM(bias.shape, F32),
        vmem((samples, LANES), F32), vmem((1, LANES), F32), vmem((SP - 1, samples, LANES), F32), vmem((SP - 1, 1, LANES), F32),
        vmem((samples // 2, LANES), F32), vmem((SP - 1, samples // 2, LANES), F32), vmem((samples // 2, LANES), F32),
        vmem((DP, samples // 2, LANES), F32),
        vmem((samples, 1, LANES), F32), vmem((TP * DP, 1, LANES), F32), vmem((1, LANES), F32),
        vmem((TP * DP, 1, LANES), F32), vmem((2, 2, TP * DP // 2, 1, LANES), F32),
        vmem((T, D), F32), vmem((C, D), F32), vmem((T, D), BF16), vmem((C, D), BF16), vmem((LANES, D), BF16),
        vmem((T, LANES), F32), vmem((T, LANES), F32),
        vmem((SP * C, 2 * LANES), BF16), vmem((T + 2 * REACH, 2 * LANES), BF16), vmem((heads, T, LANES), BF16),
        vmem((heads, T, 2 * LANES), F32), vmem((heads, T, LANES), F32),
        vmem((TP, T, width), BF16), vmem((T, cols), F32),
        dma((11,)),
        dma((2,)), dma((2,)), dma((2,)), dma((2,)), dma, dma((5,)), dma, dma((2,)), dma, dma((T // PIECE, 4)), dma((4,)),
    ]
    result = pl.pallas_call(
        functools.partial(kernel, sizes),
        out_shape=vmem((T, cols), F32),
        in_specs=[any_space] * 11,
        out_specs=pl.BlockSpec(memory_space=vmem),
        scratch_shapes=scratch,
        compiler_params=pltpu.CompilerParams(
            collective_id=0, has_side_effects=True, vmem_limit_bytes=48 * 1024 * 1024
        ),
        name="step",
    )(*(pltpu.with_memory_space_constraint(v, pltpu.HBM) for v in (
        lat[0], cond, cctx[None, :], mod.transpose(0, 2, 1), ctx[0], qw, kw.T, vw.T, ow, sink, bias
    )))
    return result[None]


def solution(mesh):
    placed = (
        P("dp", "sp", None),
        P(None, "sp"),
        P("sp"),
        P(None, "sp", ("tp", "dp")),
        P("dp", "sp", None),
        P(None, "tp"),
        P(None, "tp"),
        P(None, "tp"),
        P(None, "tp"),
        P("tp"),
        P("tp"),
    )
    sizes = (mesh.shape["sp"], mesh.shape["tp"], mesh.shape["dp"])
    return jax.shard_map(
        functools.partial(per_device, sizes),
        mesh=mesh, in_specs=placed, out_specs=P("dp", "sp", "tp"), check_vma=False,
    )
```
